32 devices in a mesh: rep: 2 (over x), fs: 8 (over z, y), tp: 2 (over core).
Axes of the slice: x: 2, y: 2, z: 4, core: 2. Of those that a mesh axis runs over, the one named last changes fastest.
Arguments:
- tokens: bfloat16 [16384, 2048], P(('rep', 'fs'), 'tp'), may hold values from -6 to 6
- attention_pre_gain: float32 [2048], replicated, may hold values from 0.1 to 1.9
- query_matrix: bfloat16 [2048, 512], P('fs', 'tp'), may hold values from -0.125 to 0.125
- key_matrix: bfloat16 [2048, 512], P('fs', 'tp'), may hold values from -0.125 to 0.125
- value_matrix: bfloat16 [2048, 1024], P('fs', 'tp'), may hold values from -0.125 to 0.125
- decay_first_weight: bfloat16 [2048, 16], replicated, may hold values from -0.125 to 0.125
- decay_second_weight: bfloat16 [16, 512], P(None, 'tp'), may hold values from -1.5 to 1.5
- decay_offset_bias: float32 [512], P('tp'), may hold values from 0 to 6
- extra_log_surge: float32 [16384, 2], P(('rep', 'fs'), 'tp'), may hold values from -0.7 to 0
- readout_head_gain: float32 [512], replicated, may hold values from 0.1 to 1.9
- output_matrix: bfloat16 [1024, 2048], P('tp', 'fs'), may hold values from -2.4375 to 2.4375
- attention_post_gain: float32 [2048], P('tp'), may hold values from 0.1 to 1.9
- feedforward_pre_gain: float32 [2048], replicated, may hold values from 0.1 to 1.9
- up_matrix: bfloat16 [2048, 4096], P('fs', 'tp'), may hold values from -0.125 to 0.125
- down_matrix: bfloat16 [4096, 2048], P('tp', 'fs'), may hold values from -1.21875 to 1.21875
- feedforward_post_gain: float32 [2048], P('tp'), may hold values from 0.1 to 1.9
Outputs:
- layer_out: bfloat16 [16384, 2048], P(('rep', 'fs'), 'tp')
The draws below stay inside these ranges and needn't reach their ends.
All inputs are finite; a program needn't handle non-finite values.
Results may differ from the reference program's by a relative error of at most 0.017.
Values may be sent and summed in bfloat16 or wider, within the bound.
A program may use at most 128 MiB of HBM per device.

```python
import jax
import jax.numpy as jnp
from jax import lax

D = 2048
FF = 4096
HEADS = 2
KEY_WIDTH = 256
DV = 512
RANK = 16
BLOCK = 64
LENGTH = 1024
KEYDIM = 512
VALDIM = 1024
TOKENS = 16384
N_TP = 2


def draw_decay_offset_bias(key, part):
    base = jax.random.fold_in(key, 11)
    first, second, third = jax.random.split(base, 3)
    slow_share = 0.5
    chosen = jax.random.uniform(first, (KEYDIM,), jnp.float32) < slow_share
    slow_value = jax.random.uniform(second, (KEYDIM,), jnp.float32, 4.0, 6.0)
    fast_value = jax.random.uniform(third, (KEYDIM,), jnp.float32, 0.0, 1.5)
    return jnp.where(chosen, slow_value, fast_value)


def draw_extra_log_surge(key, part):
    base = jax.random.fold_in(key, 23)
    first, second = jax.random.split(base, 2)
    marked = jax.random.randint(first, (TOKENS, HEADS), 0, LENGTH // 4) == 0
    sizes = jnp.log(jax.random.uniform(second, (TOKENS, HEADS), jnp.float32, 0.5, 0.8))
    return jnp.where(marked, sizes, jnp.zeros((TOKENS, HEADS), jnp.float32))


def ramped_matrix(key, rows, columns):
    first, second = jax.random.split(key, 2)
    entries = jnp.clip(jax.random.normal(first, (rows, columns), jnp.float32), -6.0, 6.0)
    top_scale = 10.0
    ramp = jnp.exp(jnp.log(top_scale) * jnp.arange(columns, dtype=jnp.float32) / columns)
    rough = jax.random.uniform(second, (columns,), jnp.float32, 0.7, 1.3)
    return (entries * rows ** (-0.5) * (ramp * rough)[None, :]).astype(jnp.bfloat16)


def draw_down_matrix(key, part):
    return ramped_matrix(jax.random.fold_in(key, 37), FF, D)


def draw_output_matrix(key, part):
    return ramped_matrix(jax.random.fold_in(key, 53), VALDIM, D)


def shard_levels(key, dims, pieces, low, high):
    factor_of, own = 1.0, jax.random.fold_in(key, 6)
    for position, parts in pieces:
        draws = jnp.exp(jax.random.uniform(jax.random.fold_in(own, position), (parts,), jnp.float32, low / len(pieces), high / len(pieces)))
        factor_of = factor_of * jnp.repeat(draws, dims[position] // parts).reshape([-1 if axis == position else 1 for axis in range(len(dims))])
    return factor_of


def bell_draw(stream_key, shape, deviation, limit, cuts=(), held_as=jnp.bfloat16):
    drawn = jax.random.normal(stream_key, shape, jnp.float32) * deviation
    if len(cuts) > 0:
        drawn = shard_levels(stream_key, shape, cuts, -0.22, 0.18) * drawn
    return jnp.clip(drawn, min=-limit, max=limit).astype(held_as)


def setup_inputs(seed: int = 0) -> dict:
    key_of = jax.random.split(jax.random.key(seed), 17)
    tokens = bell_draw(key_of[0], (TOKENS, D), 1.0, 6.0, ((0, 16), (1, 2)))
    attention_pre_gain = jnp.clip(1.0 + 0.18 * jax.random.normal(key_of[1], (D,), jnp.float32), 0.1, 1.9)
    query_matrix = bell_draw(key_of[2], (D, KEYDIM), D ** -0.5, 0.125, ((0, 8), (1, 2)))
    key_matrix = bell_draw(key_of[3], (D, KEYDIM), D ** -0.5, 0.125, ((0, 8), (1, 2)))
    value_matrix = bell_draw(key_of[4], (D, VALDIM), D ** -0.5, 0.125, ((0, 8), (1, 2)))
    decay_first_weight = bell_draw(key_of[5], (D, RANK), D ** -0.5, 0.125)
    decay_second_weight = bell_draw(key_of[6], (RANK, KEYDIM), RANK ** -0.5, 1.5, ((1, 2),))
    decay_offset_bias = draw_decay_offset_bias(jax.random.fold_in(key_of[16], 71), 0)
    extra_log_surge = draw_extra_log_surge(jax.random.fold_in(key_of[16], 71), 0)
    readout_head_gain = jnp.clip(1.0 + 0.18 * jax.random.normal(key_of[9], (DV,), jnp.float32), 0.1, 1.9)
    output_matrix = draw_output_matrix(jax.random.fold_in(key_of[16], 71), 0)
    attention_post_gain = jnp.clip(1.0 + 0.18 * jax.random.normal(key_of[11], (D,), jnp.float32), 0.1, 1.9)
    feedforward_pre_gain = jnp.clip(1.0 + 0.18 * jax.random.normal(key_of[12], (D,), jnp.float32), 0.1, 1.9)
    up_matrix = bell_draw(key_of[13], (D, FF), D ** -0.5, 0.125, ((0, 8), (1, 2)))
    down_matrix = draw_down_matrix(jax.random.fold_in(key_of[16], 71), 0)
    feedforward_post_gain = jnp.clip(1.0 + 0.18 * jax.random.normal(key_of[15], (D,), jnp.float32), 0.1, 1.9)
    return {"tokens": tokens, "attention_pre_gain": attention_pre_gain, "query_matrix": query_matrix, "key_matrix": key_matrix, "value_matrix": value_matrix, "decay_first_weight": decay_first_weight, "decay_second_weight": decay_second_weight, "decay_offset_bias": decay_offset_bias, "extra_log_surge": extra_log_surge, "readout_head_gain": readout_head_gain, "output_matrix": output_matrix, "attention_post_gain": attention_post_gain, "feedforward_pre_gain": feedforward_pre_gain, "up_matrix": up_matrix, "down_matrix": down_matrix, "feedforward_post_gain": feedforward_post_gain}


EPS = 1e-06

def pre_norm(rows, gain):
    values = rows.astype(jnp.float32)
    scale = lax.rsqrt(lax.optimization_barrier(jnp.mean(values * values, axis=-1, keepdims=True)) + EPS)
    return (values * scale * gain).astype(jnp.bfloat16)

def block_attention(queries, keys_in, values_in, log_gates):
    head_count, token_length, key_size = queries.shape
    value_size = values_in.shape[-1]
    blocks = token_length // BLOCK

    def to_blocks(array):
        return array.reshape(head_count, blocks, BLOCK, array.shape[-1]).transpose(1, 0, 2, 3)
    causal = jnp.tril(jnp.ones((BLOCK, BLOCK), dtype=bool))[None, :, :, None]
    highest = lax.Precision.HIGHEST

    def advance(memory_state, inputs):
        query_blk, key_blk, value_blk, gate_blk = inputs
        cumulative = jnp.cumsum(gate_blk, axis=1)
        carried = jnp.einsum('hid,hde->hie', query_blk * jnp.exp(cumulative), memory_state, precision=highest)
        spread_log = cumulative[:, :, None, :] - cumulative[:, None, :, :]
        weights = jnp.exp(jnp.where(causal, spread_log, -jnp.inf))
        scores = jnp.einsum('hid,hjd,hijd->hij', query_blk, key_blk, weights, precision=highest)
        readout = carried + jnp.einsum('hij,hje->hie', scores, value_blk, precision=highest)
        final_log = cumulative[:, -1:, :]
        memory_state = jnp.exp(final_log[:, 0, :])[:, :, None] * memory_state + jnp.einsum('hjd,hje->hde', key_blk * jnp.exp(final_log - cumulative), value_blk, precision=highest)
        return (memory_state, readout)
    start_state = jnp.zeros((head_count, key_size, value_size), jnp.float32)
    _, readout = lax.scan(advance, start_state, (to_blocks(queries), to_blocks(keys_in), to_blocks(values_in), to_blocks(log_gates)))
    return readout.transpose(1, 0, 2, 3).reshape(head_count, token_length, value_size)

def grouped_sum(left, right):
    group = left.shape[1] // N_TP
    total = jnp.zeros((left.shape[0], right.shape[1]), jnp.float32)
    for member in range(N_TP):
        partial_value = jnp.dot(left[:, member * group:(member + 1) * group], right[member * group:(member + 1) * group], preferred_element_type=jnp.float32)
        rounded = lax.optimization_barrier(partial_value.astype(jnp.bfloat16))
        total = total + rounded.astype(jnp.float32)
    return total

def post_add(resid, branch, gain):
    scale = lax.rsqrt(lax.optimization_barrier(jnp.mean(branch * branch, axis=-1, keepdims=True)) + EPS)
    return (resid.astype(jnp.float32) + branch * scale * gain).astype(jnp.bfloat16)

def reference(tokens, attention_pre_gain, query_matrix, key_matrix, value_matrix, decay_first_weight, decay_second_weight, decay_offset_bias, extra_log_surge, readout_head_gain, output_matrix, attention_post_gain, feedforward_pre_gain, up_matrix, down_matrix, feedforward_post_gain):
    normed = pre_norm(tokens, attention_pre_gain)
    query_proj = jnp.dot(normed, query_matrix, preferred_element_type=jnp.float32).astype(jnp.bfloat16)
    key_proj = jnp.dot(normed, key_matrix, preferred_element_type=jnp.float32).astype(jnp.bfloat16)
    value_proj = jnp.dot(normed, value_matrix, preferred_element_type=jnp.float32).astype(jnp.bfloat16)
    rank_rows = jnp.dot(normed, decay_first_weight, preferred_element_type=jnp.float32).astype(jnp.bfloat16)
    gate_source_input = jnp.dot(rank_rows, decay_second_weight, preferred_element_type=jnp.float32) + decay_offset_bias
    logarithm_decay = jax.nn.log_sigmoid(gate_source_input) / 16.0 + jnp.repeat(extra_log_surge, KEY_WIDTH, axis=1)
    sequences = TOKENS // LENGTH

    def by_head(array, size):
        return array.astype(jnp.float32).reshape(sequences, LENGTH, HEADS, size).transpose(0, 2, 1, 3)
    queries = by_head(query_proj, KEY_WIDTH) * KEY_WIDTH ** (-0.5)
    readout = lax.map(lambda group: block_attention(*group), (queries, by_head(key_proj, KEY_WIDTH), by_head(value_proj, DV), by_head(logarithm_decay, KEY_WIDTH)))
    readout = readout.transpose(0, 2, 1, 3).reshape(TOKENS, HEADS, DV)
    head_scale = lax.rsqrt(lax.optimization_barrier(jnp.mean(readout * readout, axis=-1, keepdims=True)) + EPS)
    mixed = (readout * head_scale * readout_head_gain).astype(jnp.bfloat16).reshape(TOKENS, VALDIM)
    attn = grouped_sum(mixed, output_matrix)
    resid = post_add(tokens, attn, attention_post_gain)
    normed_mid = pre_norm(resid, feedforward_pre_gain)
    hidden = jax.nn.relu(jnp.dot(normed_mid, up_matrix, preferred_element_type=jnp.float32))
    squared = (hidden * hidden).astype(jnp.bfloat16)
    feed = grouped_sum(squared, down_matrix)
    return post_add(resid, feed, feedforward_post_gain)
```

```python
import functools
import math

import jax
import jax.numpy as jnp
from jax import lax
from jax.experimental import pallas as pl
from jax.experimental.pallas import tpu as pltpu
from jax.sharding import PartitionSpec as P

KEY_WIDTH = 256
DV = 512
LENGTH = 1024
CHUNK = 128
SUB = 16
EPS = 1e-06


def pre_norm(rows, gain):
    values = rows.astype(jnp.float32)
    scale = lax.rsqrt(jnp.mean(values * values, axis=-1, keepdims=True) + EPS)
    return (values * scale * gain).astype(jnp.bfloat16)


def attend(q, k, v, rank_rows, second, bias, surge, gain, state):
    subs = CHUNK // SUB
    q = q.astype(jnp.float32) * KEY_WIDTH ** (-0.5)
    k = k.astype(jnp.float32)
    source = jnp.dot(rank_rows, second, preferred_element_type=jnp.float32) + bias
    log_sig = jnp.minimum(source, 0.0) - jnp.log1p(jnp.exp(-jnp.abs(source)))
    gate = log_sig / 16.0 + surge

    row = lax.broadcasted_iota(jnp.int32, (CHUNK, CHUNK), 0)
    col = lax.broadcasted_iota(jnp.int32, (CHUNK, CHUNK), 1)
    lower = (row >= col).astype(jnp.float32)
    cum = jnp.dot(
        lower, gate, preferred_element_type=jnp.float32, precision=lax.Precision.HIGHEST
    )

    q3 = q.reshape(subs, SUB, KEY_WIDTH)
    k3 = k.reshape(subs, SUB, KEY_WIDTH)
    c3 = cum.reshape(subs, SUB, KEY_WIDTH)
    pick_col = lax.rem(lax.broadcasted_iota(jnp.int32, (KEY_WIDTH, CHUNK), 1), SUB)
    scores = jnp.zeros((CHUNK, CHUNK), jnp.float32)
    for j in range(SUB):
        weight = jnp.exp(jnp.minimum(c3 - c3[:, j : j + 1, :], 0.0))
        term = (q3 * k3[:, j : j + 1, :] * weight).reshape(CHUNK, KEY_WIDTH)
        scores += jnp.dot(
            term.astype(jnp.bfloat16),
            (pick_col == j).astype(jnp.bfloat16),
            preferred_element_type=jnp.float32,
        )
    scores = jnp.where((row // SUB == col // SUB) & (row >= col), scores, 0.0)

    pieces = [jnp.zeros((SUB, CHUNK), jnp.float32)]
    key_row = lax.broadcasted_iota(jnp.int32, (CHUNK, KEY_WIDTH), 0)
    for i in range(1, subs):
        edge = cum[i * SUB - 1 : i * SUB, :]
        left = q3[i] * jnp.exp(jnp.minimum(c3[i] - edge, 0.0))
        right = jnp.where(key_row < i * SUB, k * jnp.exp(jnp.minimum(edge - cum, 0.0)), 0.0)
        pieces.append(
            lax.dot_general(
                left.astype(jnp.bfloat16),
                right.astype(jnp.bfloat16),
                (((1,), (1,)), ((), ())),
                preferred_element_type=jnp.float32,
            )
        )
    scores = scores + jnp.concatenate(pieces, axis=0)

    last = cum[CHUNK - 1 : CHUNK, :]
    held = state[...]
    readout = lax.dot_general(
        (q * jnp.exp(cum)).astype(jnp.bfloat16),
        held.astype(jnp.bfloat16),
        (((1,), (1,)), ((), ())),
        preferred_element_type=jnp.float32,
    ) + jnp.dot(scores.astype(jnp.bfloat16), v, preferred_element_type=jnp.float32)
    faded = (k * jnp.exp(jnp.minimum(last - cum, 0.0))).astype(jnp.bfloat16)
    state[...] = held * jnp.exp(last) + lax.dot_general(
        v, faded, (((0,), (0,)), ((), ())), preferred_element_type=jnp.float32
    )
    scale = lax.rsqrt(jnp.mean(readout * readout, axis=-1, keepdims=True) + EPS)
    return (readout * scale * gain).astype(jnp.bfloat16)


def attention_kernel(
    q_ref, k_ref, v_ref, rank_ref, second_ref, bias_ref, surge_ref, gain_ref, o_ref, state
):
    @pl.when(lax.rem(pl.program_id(1), LENGTH // CHUNK) == 0)
    def _():
        state[...] = jnp.zeros_like(state)

    o_ref[...] = attend(
        q_ref[...], k_ref[...], v_ref[...], rank_ref[...], second_ref[...], bias_ref[...],
        surge_ref[0], gain_ref[...], state,
    )


def attention(qkv, rank_rows, second, bias, surge, gain):
    tokens = qkv.shape[0]
    heads = second.shape[1] // KEY_WIDTH
    rank = rank_rows.shape[1]
    value_base = 2 * heads * KEY_WIDTH // DV
    return pl.pallas_call(
        attention_kernel,
        grid=(heads, tokens // CHUNK),
        in_specs=[
            pl.BlockSpec((CHUNK, KEY_WIDTH), lambda h, c: (c, h)),
            pl.BlockSpec((CHUNK, KEY_WIDTH), lambda h, c: (c, heads + h)),
            pl.BlockSpec((CHUNK, DV), lambda h, c: (c, value_base + h)),
            pl.BlockSpec((CHUNK, rank), lambda h, c: (c, 0)),
            pl.BlockSpec((rank, KEY_WIDTH), lambda h, c: (0, h)),
            pl.BlockSpec((1, KEY_WIDTH), lambda h, c: (0, h)),
            pl.BlockSpec((1, CHUNK, 1), lambda h, c: (h, c, 0)),
            pl.BlockSpec((1, DV), lambda h, c: (0, 0)),
        ],
        out_specs=pl.BlockSpec((CHUNK, DV), lambda h, c: (c, h)),
        out_shape=jax.ShapeDtypeStruct((tokens, heads * DV), jnp.bfloat16),
        scratch_shapes=[pltpu.VMEM((DV, KEY_WIDTH), jnp.float32)],
        compiler_params=pltpu.CompilerParams(
            dimension_semantics=("arbitrary", "arbitrary"), vmem_limit_bytes=24 * 2**20
        ),
        cost_estimate=pl.CostEstimate(
            flops=20_000_000_000, bytes_accessed=20_000_000, transcendentals=8_000_000
        ),
        name="attention",
    )(qkv, qkv, qkv, rank_rows, second, bias[None, :], surge.T[:, :, None], gain[None, :])


def on_device(
    n_rep,
    n_fs,
    n_tp,
    tokens,
    attention_pre_gain,
    query_matrix,
    key_matrix,
    value_matrix,
    decay_first_weight,
    decay_second_weight,
    decay_offset_bias,
    extra_log_surge,
    readout_head_gain,
    output_matrix,
    attention_post_gain,
    feedforward_pre_gain,
    up_matrix,
    down_matrix,
    feedforward_post_gain,
):
    me = lax.axis_index("tp")
    rep = lax.axis_index("rep")
    swap = [(i, 1 - i) for i in range(2)]

    def both_halves(mine):
        if n_tp != 2:
            return lax.all_gather(mine, "tp", axis=1, tiled=True)
        other = lax.ppermute(mine, "tp", swap)
        first = me == 0
        return jnp.concatenate(
            [jnp.where(first, mine, other), jnp.where(first, other, mine)], axis=1
        )

    def sum_scattered(partial):
        if n_tp != 2:
            return lax.psum_scatter(partial, "tp", scatter_dimension=1, tiled=True).astype(
                jnp.float32
            )
        size = partial.shape[1] // 2
        keep = lax.dynamic_slice_in_dim(partial, me * size, size, 1)
        send = lax.dynamic_slice_in_dim(partial, (1 - me) * size, size, 1)
        return keep.astype(jnp.float32) + lax.ppermute(send, "tp", swap).astype(jnp.float32)

    def summed(rows):
        if n_tp != 2:
            return lax.psum(rows, "tp")
        return rows + lax.ppermute(rows, "tp", swap)

    def part(weight, axis):
        size = weight.shape[axis] // n_rep
        return lax.dynamic_slice_in_dim(weight, rep * size, size, axis)

    weights = jnp.concatenate([query_matrix, key_matrix, value_matrix], axis=1)
    with jax.named_scope("gather_in"):
        whole_in = lax.all_gather(weights, "fs", axis=0, tiled=True)
    with jax.named_scope("gather_out"):
        whole_out = lax.all_gather(output_matrix, "fs", axis=1, tiled=True)
    rows = up_matrix.shape[0]
    cols = down_matrix.shape[1]
    mine = lax.axis_index("fs")
    place = jnp.where(mine % 2 == 0, mine // 2, n_fs - 1 - mine // 2)
    cycle = [2 * p if p < n_fs // 2 else 2 * (n_fs - 1 - p) + 1 for p in range(n_fs)]
    ahead = [(cycle[p], cycle[(p + 1) % n_fs]) for p in range(n_fs)]
    behind = [(to, at) for at, to in ahead]

    def shard_at(p):
        p = (p + n_fs) % n_fs
        return jnp.where(p < n_fs // 2, 2 * p, 2 * (n_fs - 1 - p) + 1)

    def travel(own, hops_ahead, hops_behind):
        chunks = []
        for hops, ring, sign in ((hops_ahead, ahead, -1), (hops_behind, behind, 1)):
            piece = own
            for step in range(1, hops + 1):
                piece = lax.ppermute(piece, "fs", ring)
                chunks.append((step, shard_at(place + sign * step), piece))
        chunks.sort(key=lambda c: c[0])
        pieces = [(piece, rep, shard) for _, shard, piece in chunks]
        others = []
        for piece, _, shard in pieces:
            for turn in range(1, n_rep):
                other = lax.ppermute(
                    piece, "rep", [(r, (r + turn) % n_rep) for r in range(n_rep)]
                )
                others.append((other, (rep + n_rep - turn) % n_rep, shard))
        return pieces, others

    def hold_until(value, moved):
        tied = lax.optimization_barrier((value, *[m[0] for m in moved]))
        return tied[0], [(t, *m[1:]) for t, m in zip(tied[1:], moved)]

    up_cols = up_matrix.shape[1] // n_rep
    down_rows = down_matrix.shape[0] // n_rep
    half = n_fs // 2
    up_pieces, up_others = travel(part(up_matrix, 1), half, n_fs - 1 - half)
    with jax.named_scope("gather_down"):
        whole_down = lax.all_gather(down_matrix, "fs", axis=1, tiled=True)

    gathered = both_halves(tokens)
    width = gathered.shape[1]
    normed = pre_norm(gathered, attention_pre_gain)
    rank_rows = jnp.dot(normed, decay_first_weight, preferred_element_type=jnp.float32).astype(
        jnp.bfloat16
    )
    early = up_pieces + up_others[: half]
    normed, early = hold_until(normed, early)
    with jax.named_scope("project"):
        qkv = jnp.dot(normed, whole_in, preferred_element_type=jnp.float32).astype(jnp.bfloat16)
    with jax.named_scope("mix"):
        mixed = attention(
            qkv, rank_rows, decay_second_weight, decay_offset_bias, extra_log_surge,
            readout_head_gain,
        )
    mixed, late = hold_until(mixed, up_others[half :])
    with jax.named_scope("out_project"):
        partial_attn = jnp.dot(mixed, whole_out, preferred_element_type=jnp.float32)
    attn = sum_scattered(partial_attn.astype(jnp.bfloat16))
    attn_total = summed(jnp.sum(attn * attn, axis=1))
    attn_scale = lax.rsqrt(attn_total / width + EPS)[:, None]
    resid = (tokens.astype(jnp.float32) + attn * attn_scale * attention_post_gain).astype(
        jnp.bfloat16
    )
    normed_mid = pre_norm(both_halves(resid), feedforward_pre_gain)
    whole_up = lax.dynamic_update_slice(
        jnp.zeros((n_fs * rows, up_matrix.shape[1]), jnp.bfloat16), up_matrix, (mine * rows, 0)
    )
    for piece, r, j in early + late:
        whole_up = lax.dynamic_update_slice(whole_up, piece, (j * rows, r * up_cols))
    hidden = jax.nn.relu(jnp.dot(normed_mid, whole_up, preferred_element_type=jnp.float32))
    squared = (hidden * hidden).astype(jnp.bfloat16)
    partial_feed = jnp.dot(squared, whole_down, preferred_element_type=jnp.float32)
    feed = sum_scattered(partial_feed.astype(jnp.bfloat16))
    feed_total = summed(jnp.sum(feed * feed, axis=1))
    feed_scale = lax.rsqrt(feed_total / width + EPS)[:, None]
    return (resid.astype(jnp.float32) + feed * feed_scale * feedforward_post_gain).astype(
        jnp.bfloat16
    )


MESH = pl.DeviceIdType.MESH
UNIT = 16


def ring_split(rows, heavy_x):
    third = rows / (3 * UNIT)
    a = (math.ceil(third) if heavy_x else math.floor(third)) * UNIT
    return a, rows - 2 * a


def layer_kernel(
    dims,
    tok_hbm,
    pre_gain,
    wq_hbm,
    wk_hbm,
    wv_hbm,
    first_ref,
    second_ref,
    bias_ref,
    surge_ref,
    head_gain,
    out_hbm,
    post_gain,
    mid_gain,
    up_hbm,
    down_hbm,
    last_gain,
    o_ref,
    wqkv,
    wout,
    wup,
    wdn,
    tok,
    normed,
    rank,
    qkv,
    mixed,
    keep,
    sendb,
    recvb,
    ss,
    ss_in,
    ss2,
    ss2_in,
    sq,
    fbuf,
    rbuf,
    state,
    local_sem,
    ring_send,
    ring_recv,
    x_send,
    x_recv,
    core_send,
    core_recv,
    feed_send,
    feed_recv,
):
    n_fs = dims["fs"]
    half_ring = n_fs // 2
    rep, fs, tp = lax.axis_index("rep"), lax.axis_index("fs"), lax.axis_index("tp")
    place = jnp.where(lax.rem(fs, 2) == 0, fs // 2, n_fs - 1 - fs // 2)

    def shard_at(p):
        p = lax.rem(p + 2 * n_fs, n_fs)
        return jnp.where(p < half_ring, 2 * p, 2 * (n_fs - 1 - p) + 1)

    ring_id = [{"fs": shard_at(place + 1)}, {"fs": shard_at(place - 1)}]
    x_id = {"rep": 1 - rep}
    core_id = {"tp": 1 - tp}

    tokens, width = normed.shape
    dh = tok.shape[2]
    qkv_rows = wq_hbm.shape[0]
    out_rows = out_hbm.shape[0]
    up_rows = up_hbm.shape[0]
    up_half = up_hbm.shape[1] // 2
    dn_half = down_hbm.shape[0] // 2
    cols = down_hbm.shape[1]
    per_half = n_fs // 2

    def rows_of(ref, shard_rows, lanes):
        def view(j, off, n):
            return ref.at[pl.ds(pl.multiple_of(j * shard_rows + off, UNIT), n), lanes]

        return view

    def slab_of(ref, base):
        def view(j, off, n):
            return ref.at[j, pl.ds(pl.multiple_of(base + off, UNIT), n), :]

        return view

    streams = [
        (rows_of(wqkv, qkv_rows, slice(None)), qkv_rows // 2, ring_split(qkv_rows // 2, True)),
        (slab_of(wout, 0), out_rows // 2, ring_split(out_rows // 2, False)),
        (rows_of(wup, up_rows, slice(0, up_half)), up_rows // 2, ring_split(up_rows // 2, True)),
        (
            rows_of(wup, up_rows, slice(up_half, 2 * up_half)),
            up_rows // 2,
            ring_split(up_rows // 2, False),
        ),
        (slab_of(wdn, 0), dn_half // 2, ring_split(dn_half // 2, False)),
        (slab_of(wdn, dn_half), dn_half // 2, ring_split(dn_half // 2, True)),
    ]
    QKV, OUT, UP0, UP1, DN0, DN1 = range(6)

    def sign(d):
        return 1 - 2 * d

    def chunk_of(e, d):
        return e + d - 2 * e * d

    def ring_copy(s, d, e, h, own_send):
        view, rows, (a, c) = streams[s]
        step = h - 1 if own_send else h
        j = shard_at(place - sign(d) * step)
        piece = view(j, chunk_of(e, d) * rows + rep * a, a + c)
        return pltpu.make_async_remote_copy(
            src_ref=piece,
            dst_ref=piece,
            send_sem=ring_send.at[s, d, e, h - 1],
            recv_sem=ring_recv.at[s, d, e, h - 1],
            device_id=ring_id[d],
            device_id_type=MESH,
        )

    def x_copy(s, d, e, h, own_send):
        view, rows, (a, c) = streams[s]
        j = shard_at(place - sign(d) * h)
        side = rep if own_send else 1 - rep
        piece = view(j, chunk_of(e, d) * rows + side * (a + c), a)
        return pltpu.make_async_remote_copy(
            src_ref=piece,
            dst_ref=piece,
            send_sem=x_send.at[s, d, e, h - 1],
            recv_sem=x_recv.at[s, d, e, h - 1],
            device_id=x_id,
            device_id_type=MESH,
        )

    n_items = n_fs - 1

    def begin(s):
        for e in range(2):
            for d in range(2):
                ring_copy(s, d, e, 1, True).start()

    def poll(s, i):
        if isinstance(i, int):
            e, h = i % 2, i // 2 + 1
        else:
            e = lax.rem(i, 2)
            h = i // 2 + 1
        for d in range(2):
            ring_copy(s, d, e, h, False).wait_recv()
            if isinstance(i, int):
                if i + 2 < n_items:
                    ring_copy(s, d, e, h + 1, True).start()
            else:

                @pl.when(i + 2 < n_items)
                def _():
                    ring_copy(s, d, e, h + 1, True).start()

            x_copy(s, d, e, h, True).start()

    def all_items():
        for i in range(n_items):
            for d in range(2):
                yield d, i % 2, i // 2 + 1

    def x_wait(s):
        for d, e, h in all_items():
            x_copy(s, d, e, h, False).wait_recv()

    head_cols = wq_hbm.shape[1]
    own = [
        pltpu.make_async_copy(
            wq_hbm,
            wqkv.at[pl.ds(pl.multiple_of(fs * qkv_rows, UNIT), qkv_rows), 0:head_cols],
            local_sem.at[0],
        ),
        pltpu.make_async_copy(
            wk_hbm,
            wqkv.at[
                pl.ds(pl.multiple_of(fs * qkv_rows, UNIT), qkv_rows), head_cols : 2 * head_cols
            ],
            local_sem.at[1],
        ),
        pltpu.make_async_copy(
            wv_hbm,
            wqkv.at[pl.ds(pl.multiple_of(fs * qkv_rows, UNIT), qkv_rows), 2 * head_cols :],
            local_sem.at[2],
        ),
        pltpu.make_async_copy(tok_hbm, tok.at[tp], local_sem.at[3]),
        pltpu.make_async_copy(out_hbm, wout.at[fs], local_sem.at[4]),
        pltpu.make_async_copy(
            up_hbm,
            wup.at[pl.ds(pl.multiple_of(fs * up_rows, UNIT), up_rows), :],
            local_sem.at[5],
        ),
        pltpu.make_async_copy(down_hbm, wdn.at[fs], local_sem.at[6]),
    ]
    for copy in own:
        copy.start()

    barrier = pltpu.get_barrier_semaphore()
    for target in (*ring_id, x_id, core_id):
        pl.semaphore_signal(barrier, inc=1, device_id=target, device_id_type=MESH)
    pl.semaphore_wait(barrier, 4)

    for copy in own[:3]:
        copy.wait()
    begin(QKV)

    def core_copy(k, src, dst):
        return pltpu.make_async_remote_copy(
            src_ref=src,
            dst_ref=dst,
            send_sem=core_send.at[k],
            recv_sem=core_recv.at[k],
            device_id=core_id,
            device_id_type=MESH,
        )

    own[3].wait()
    swap_tok = core_copy(0, tok.at[tp], tok.at[tp])
    swap_tok.start()
    for copy in own[4:]:
        copy.wait()
    core_copy(0, tok.at[1 - tp], tok.at[1 - tp]).wait_recv()

    def norm_rows(gain, count):
        def body(r, carry):
            at = pl.ds(pl.multiple_of(r * count, count), count)
            left = tok[0, at, :].astype(jnp.float32)
            right = tok[1, at, :].astype(jnp.float32)
            total = jnp.sum(left * left, axis=1, keepdims=True) + jnp.sum(
                right * right, axis=1, keepdims=True
            )
            scale = lax.rsqrt(total / width + EPS)
            normed[at, 0:dh] = (left * scale * gain[:, 0:dh]).astype(jnp.bfloat16)
            normed[at, dh:] = (right * scale * gain[:, dh:]).astype(jnp.bfloat16)
            return carry

        lax.fori_loop(0, tokens // count, body, 0)

    norm_rows(pre_gain, 64)
    poll(QKV, 0)

    def rank_body(r, carry):
        at = pl.ds(pl.multiple_of(r * 256, 256), 256)
        rank[at, :] = jnp.dot(
            normed[at, :], first_ref[...], preferred_element_type=jnp.float32
        ).astype(jnp.bfloat16)
        return carry

    lax.fori_loop(0, tokens // 256, rank_body, 0)
    for i in range(1, n_items):
        poll(QKV, i)
        if i == n_items - 3:
            begin(OUT)

    poll(OUT, 0)
    poll(OUT, 1)
    x_wait(QKV)

    def project(first, count):
        def body(r, carry):
            at = pl.ds(pl.multiple_of(r * 256, 256), 256)
            lanes = qkv.shape[1] // 2
            for b in range(2):
                qkv[at, b * lanes : (b + 1) * lanes] = jnp.dot(
                    normed[at, :],
                    wqkv[:, b * lanes : (b + 1) * lanes],
                    preferred_element_type=jnp.float32,
                ).astype(jnp.bfloat16)
            return carry

        lax.fori_loop(first, first + count, body, 0)

    project(0, 2)
    poll(OUT, 2)
    poll(OUT, 3)
    project(2, tokens // 256 - 2)
    for i in range(4, n_items):
        poll(OUT, i)
        if i == n_items - 3:
            begin(UP0)

    chunks = tokens // CHUNK

    def attention_chunk(chunk, carry):
        @pl.when(chunk < n_items)
        def _():
            poll(UP0, chunk)

        @pl.when(chunk == n_items - 3)
        def _():
            begin(UP1)

        @pl.when(lax.rem(chunk, LENGTH // CHUNK) == 0)
        def _():
            state[...] = jnp.zeros_like(state)

        at = pl.ds(pl.multiple_of(chunk * CHUNK, CHUNK), CHUNK)
        surge_all = surge_ref[...]
        lane = lax.broadcasted_iota(jnp.int32, surge_all.shape, 1)
        surge = jnp.sum(jnp.where(lane == chunk, surge_all, 0.0), axis=1, keepdims=True)
        mixed[at, :] = attend(
            qkv[at, 0:head_cols],
            qkv[at, head_cols : 2 * head_cols],
            qkv[at, 2 * head_cols :],
            rank[at, :],
            second_ref[...],
            bias_ref[...],
            surge,
            head_gain[...],
            state,
        )
        return carry

    lax.fori_loop(0, chunks, attention_chunk, 0)

    poll(UP1, 0)
    x_wait(OUT)

    def out_rows_body(r, carry):
        at = pl.ds(pl.multiple_of(r * 256, 256), 256)
        rows = mixed[at, :]
        for k in range(per_half):
            keep[at, k * cols : (k + 1) * cols] = jnp.dot(
                rows, wout[tp * per_half + k], preferred_element_type=jnp.float32
            ).astype(jnp.bfloat16)
            sendb[at, k * cols : (k + 1) * cols] = jnp.dot(
                rows, wout[(1 - tp) * per_half + k], preferred_element_type=jnp.float32
            ).astype(jnp.bfloat16)
        return carry

    lax.fori_loop(0, tokens // 256, out_rows_body, 0)
    poll(UP1, 1)
    core_copy(1, sendb, recvb).start()
    poll(UP1, 2)
    core_copy(1, sendb, recvb).wait_recv()

    def attn_rows(r, count):
        at = pl.ds(pl.multiple_of(r * count, count), count)
        return at, keep[at, :].astype(jnp.float32) + recvb[at, :].astype(jnp.float32)

    def square_body(r, carry):
        at, attn = attn_rows(r, 64)
        ss[at, :] = jnp.broadcast_to(
            jnp.sum(attn * attn, axis=1, keepdims=True), (64, ss.shape[1])
        )
        return carry

    lax.fori_loop(0, tokens // 64, square_body, 0)
    poll(UP1, 3)
    core_copy(2, ss, ss_in).start()
    poll(UP1, 4)
    begin(DN0)
    core_copy(2, ss, ss_in).wait_recv()

    def resid_body(r, carry):
        at, attn = attn_rows(r, 64)
        total = ss[at, 0:1] + ss_in[at, 0:1]
        scale = lax.rsqrt(total / width + EPS)
        tok[tp, at, :] = (
            tok[tp, at, :].astype(jnp.float32) + attn * scale * post_gain[...]
        ).astype(jnp.bfloat16)
        return carry

    swap_tok.wait_send()
    lax.fori_loop(0, tokens // 64, resid_body, 0)
    poll(UP1, 5)
    swap_resid = core_copy(3, tok.at[tp], tok.at[tp])
    swap_resid.start()
    poll(UP1, 6)
    core_copy(3, tok.at[1 - tp], tok.at[1 - tp]).wait_recv()
    norm_rows(mid_gain, 64)
    x_wait(UP0)
    x_wait(UP1)

    blocks = 8
    hidden_cols = wup.shape[1] // blocks

    def up_body(b, carry):
        @pl.when(b < n_items)
        def _():
            poll(DN0, b)

        @pl.when(b == n_items - 3)
        def _():
            begin(DN1)

        lanes = pl.ds(pl.multiple_of(b * hidden_cols, hidden_cols), hidden_cols)
        for r in range(tokens // 256):
            at = slice(r * 256, (r + 1) * 256)
            hidden = jnp.maximum(
                jnp.dot(normed[at, :], wup[:, lanes], preferred_element_type=jnp.float32), 0.0
            )
            sq[at, lanes] = (hidden * hidden).astype(jnp.bfloat16)
        return carry

    lax.fori_loop(0, blocks, up_body, 0)
    x_wait(DN0)

    def feed_copy(k):
        return pltpu.make_async_remote_copy(
            src_ref=fbuf.at[(1 - tp) * per_half + k],
            dst_ref=rbuf.at[k],
            send_sem=feed_send.at[k],
            recv_sem=feed_recv.at[k],
            device_id=core_id,
            device_id_type=MESH,
        )

    def shard_of(t):
        h = (t + 1) // 2
        d = 1 - lax.rem(t, 2)
        return shard_at(place - sign(d) * h), d, h

    def down_of(t):
        j, _, _ = shard_of(t)

        def body(r, carry):
            at = pl.ds(pl.multiple_of(r * 512, 512), 512)
            fbuf[j, at, :] = jnp.dot(
                sq[at, :], wdn[j], preferred_element_type=jnp.float32
            ).astype(jnp.bfloat16)
            return carry

        lax.fori_loop(0, tokens // 512, body, 0)

    def send_of(t):
        j, _, _ = shard_of(t)

        @pl.when(j // per_half != tp)
        def _():
            feed_copy(lax.rem(j, per_half)).start()

    def down_body(i, carry):
        @pl.when(i < n_items)
        def _():
            poll(DN1, i)

        @pl.when((i >= 2) & (i < n_fs))
        def _():
            _, d, h = shard_of(i - 1)
            x_copy(DN1, d, 0, h, False).wait_recv()
            x_copy(DN1, d, 1, h, False).wait_recv()

        @pl.when(i == n_fs)
        def _():
            x_copy(DN1, 0, 0, half_ring, False).wait_recv()
            x_copy(DN1, 1, 0, half_ring, False).wait_recv()

        @pl.when(i >= 1)
        def _():
            down_of(i - 1)

        @pl.when(i >= 2)
        def _():
            send_of(i - 2)

        return carry

    lax.fori_loop(0, n_fs + 1, down_body, 0)
    send_of(n_fs - 1)
    for k in range(per_half):
        feed_copy(k).wait_recv()

    def feed_rows(r, count, k):
        at = pl.ds(pl.multiple_of(r * count, count), count)
        return at, fbuf[tp * per_half + k, at, :].astype(jnp.float32) + rbuf[k, at, :].astype(
            jnp.float32
        )

    def feed_square(r, carry):
        total = jnp.zeros((64, 1), jnp.float32)
        for k in range(per_half):
            at, feed = feed_rows(r, 64, k)
            total += jnp.sum(feed * feed, axis=1, keepdims=True)
        ss2[at, :] = jnp.broadcast_to(total, (64, ss2.shape[1]))
        return carry

    lax.fori_loop(0, tokens // 64, feed_square, 0)
    core_copy(4, ss2, ss2_in).start()
    core_copy(4, ss2, ss2_in).wait_recv()

    def last_body(r, carry):
        at = pl.ds(pl.multiple_of(r * 64, 64), 64)
        scale = lax.rsqrt((ss2[at, 0:1] + ss2_in[at, 0:1]) / width + EPS)
        for k in range(per_half):
            _, feed = feed_rows(r, 64, k)
            lanes = slice(k * cols, (k + 1) * cols)
            o_ref[at, lanes] = (
                tok[tp, at, lanes].astype(jnp.float32) + feed * scale * last_gain[:, lanes]
            ).astype(jnp.bfloat16)
        return carry

    lax.fori_loop(0, tokens // 64, last_body, 0)

    for s in range(len(streams)):
        for d, e, h in all_items():
            ring_copy(s, d, e, h, True).wait_send()
            x_copy(s, d, e, h, True).wait_send()
    core_copy(1, sendb, recvb).wait_send()
    core_copy(2, ss, ss_in).wait_send()
    swap_resid.wait_send()
    core_copy(4, ss2, ss2_in).wait_send()
    for k in range(per_half):
        feed_copy(k).wait_send()


def fused_layer(
    n_rep,
    n_fs,
    n_tp,
    tokens,
    attention_pre_gain,
    query_matrix,
    key_matrix,
    value_matrix,
    decay_first_weight,
    decay_second_weight,
    decay_offset_bias,
    extra_log_surge,
    readout_head_gain,
    output_matrix,
    attention_post_gain,
    feedforward_pre_gain,
    up_matrix,
    down_matrix,
    feedforward_post_gain,
):
    rows, dh = tokens.shape
    width = dh * n_tp
    qkv_cols = query_matrix.shape[1] + key_matrix.shape[1] + value_matrix.shape[1]
    hidden = up_matrix.shape[1]
    cols = down_matrix.shape[1]
    bf = jnp.bfloat16
    any_spec = pl.BlockSpec(memory_space=pl.ANY)
    vmem = pl.BlockSpec(memory_space=pltpu.VMEM)
    dma = pltpu.SemaphoreType.DMA
    chunks = rows // CHUNK
    surge = extra_log_surge.reshape(chunks, CHUNK).T
    return pl.pallas_call(
        functools.partial(layer_kernel, {"fs": n_fs}),
        out_shape=jax.ShapeDtypeStruct((rows, dh), bf),
        in_specs=[
            any_spec, vmem, any_spec, any_spec, any_spec, vmem, vmem, vmem, vmem, vmem,
            any_spec, vmem, vmem, any_spec, any_spec, vmem,
        ],
        out_specs=vmem,
        scratch_shapes=[
            pltpu.VMEM((width, qkv_cols), bf),
            pltpu.VMEM((n_fs, output_matrix.shape[0], cols), bf),
            pltpu.VMEM((width, hidden), bf),
            pltpu.VMEM((n_fs, hidden, cols), bf),
            pltpu.VMEM((n_tp, rows, dh), bf),
            pltpu.VMEM((rows, width), bf),
            pltpu.VMEM((rows, decay_first_weight.shape[1]), bf),
            pltpu.VMEM((rows, qkv_cols), bf),
            pltpu.VMEM((rows, DV), bf),
            pltpu.VMEM((rows, dh), bf),
            pltpu.VMEM((rows, dh), bf),
            pltpu.VMEM((rows, dh), bf),
            pltpu.VMEM((rows, 128), jnp.float32),
            pltpu.VMEM((rows, 128), jnp.float32),
            pltpu.VMEM((rows, 128), jnp.float32),
            pltpu.VMEM((rows, 128), jnp.float32),
            pltpu.VMEM((rows, hidden), bf),
            pltpu.VMEM((n_fs, rows, cols), bf),
            pltpu.VMEM((n_fs // 2, rows, cols), bf),
            pltpu.VMEM((DV, KEY_WIDTH), jnp.float32),
            dma((7,)),
            dma((6, 2, 2, n_fs // 2)),
            dma((6, 2, 2, n_fs // 2)),
            dma((6, 2, 2, n_fs // 2)),
            dma((6, 2, 2, n_fs // 2)),
            dma((5,)),
            dma((5,)),
            dma((n_fs // 2,)),
            dma((n_fs // 2,)),
        ],
        compiler_params=pltpu.CompilerParams(
            collective_id=0, has_side_effects=True, vmem_limit_bytes=60 * 2**20
        ),
        name="layer",
    )(
        tokens,
        attention_pre_gain[None, :],
        query_matrix,
        key_matrix,
        value_matrix,
        decay_first_weight,
        decay_second_weight,
        decay_offset_bias[None, :],
        surge,
        readout_head_gain[None, :],
        output_matrix,
        attention_post_gain[None, :],
        feedforward_pre_gain[None, :],
        up_matrix,
        down_matrix,
        feedforward_post_gain[None, :],
    )


def per_device(n_rep, n_fs, n_tp, *args):
    tokens, query, second, out, up, down = args[0], args[2], args[6], args[10], args[13], args[14]
    fits = (
        n_rep == 2
        and n_tp == 2
        and n_fs % 2 == 0
        and 4 <= n_fs <= 8
        and tokens.shape[0] % LENGTH == 0
        and tokens.shape[0] // CHUNK == n_fs
        and second.shape[1] == KEY_WIDTH
        and out.shape[1] % 128 == 0
        and query.shape[0] % (8 * UNIT) == 0
        and up.shape[0] % (8 * UNIT) == 0
        and down.shape[1] == out.shape[1]
    )
    return (fused_layer if fits else on_device)(n_rep, n_fs, n_tp, *args)


def solution(mesh):
    return jax.shard_map(
        functools.partial(per_device, mesh.shape["rep"], mesh.shape["fs"], mesh.shape["tp"]),
        mesh=mesh,
        in_specs=(
            P(("rep", "fs"), "tp"),
            P(),
            P("fs", "tp"),
            P("fs", "tp"),
            P("fs", "tp"),
            P(),
            P(None, "tp"),
            P("tp"),
            P(("rep", "fs"), "tp"),
            P(),
            P("tp", "fs"),
            P("tp"),
            P(),
            P("fs", "tp"),
            P("tp", "fs"),
            P("tp"),
        ),
        out_specs=P(("rep", "fs"), "tp"),
        check_vma=False,
    )
```

```python
import functools
import math

import jax
import jax.numpy as jnp
from jax import lax
from jax.experimental import pallas as pl
from jax.experimental.pallas import tpu as pltpu
from jax.sharding import PartitionSpec as P

KEY_WIDTH = 256
DV = 512
LENGTH = 1024
CHUNK = 128
SUB = 16
EPS = 1e-06


def pre_norm(rows, gain):
    values = rows.astype(jnp.float32)
    scale = lax.rsqrt(jnp.mean(values * values, axis=-1, keepdims=True) + EPS)
    return (values * scale * gain).astype(jnp.bfloat16)


def attend(q, k, v, rank_rows, second, bias, surge, gain, state):
    subs = CHUNK // SUB
    q = q.astype(jnp.float32) * KEY_WIDTH ** (-0.5)
    k = k.astype(jnp.float32)
    source = jnp.dot(rank_rows, second, preferred_element_type=jnp.float32) + bias
    log_sig = jnp.minimum(source, 0.0) - jnp.log1p(jnp.exp(-jnp.abs(source)))
    gate = log_sig / 16.0 + surge

    row = lax.broadcasted_iota(jnp.int32, (CHUNK, CHUNK), 0)
    col = lax.broadcasted_iota(jnp.int32, (CHUNK, CHUNK), 1)
    lower = (row >= col).astype(jnp.float32)
    cum = jnp.dot(
        lower, gate, preferred_element_type=jnp.float32, precision=lax.Precision.HIGHEST
    )

    q3 = q.reshape(subs, SUB, KEY_WIDTH)
    k3 = k.reshape(subs, SUB, KEY_WIDTH)
    c3 = cum.reshape(subs, SUB, KEY_WIDTH)
    pick_col = lax.rem(lax.broadcasted_iota(jnp.int32, (KEY_WIDTH, CHUNK), 1), SUB)
    scores = jnp.zeros((CHUNK, CHUNK), jnp.float32)
    for j in range(SUB):
        weight = jnp.exp(jnp.minimum(c3 - c3[:, j : j + 1, :], 0.0))
        term = (q3 * k3[:, j : j + 1, :] * weight).reshape(CHUNK, KEY_WIDTH)
        scores += jnp.dot(
            term.astype(jnp.bfloat16),
            (pick_col == j).astype(jnp.bfloat16),
            preferred_element_type=jnp.float32,
        )
    scores = jnp.where((row // SUB == col // SUB) & (row >= col), scores, 0.0)

    pieces = [jnp.zeros((SUB, CHUNK), jnp.float32)]
    key_row = lax.broadcasted_iota(jnp.int32, (CHUNK, KEY_WIDTH), 0)
    for i in range(1, subs):
        edge = cum[i * SUB - 1 : i * SUB, :]
        left = q3[i] * jnp.exp(jnp.minimum(c3[i] - edge, 0.0))
        right = jnp.where(key_row < i * SUB, k * jnp.exp(jnp.minimum(edge - cum, 0.0)), 0.0)
        pieces.append(
            lax.dot_general(
                left.astype(jnp.bfloat16),
                right.astype(jnp.bfloat16),
                (((1,), (1,)), ((), ())),
                preferred_element_type=jnp.float32,
            )
        )
    scores = scores + jnp.concatenate(pieces, axis=0)

    last = cum[CHUNK - 1 : CHUNK, :]
    held = state[...]
    readout = lax.dot_general(
        (q * jnp.exp(cum)).astype(jnp.bfloat16),
        held.astype(jnp.bfloat16),
        (((1,), (1,)), ((), ())),
        preferred_element_type=jnp.float32,
    ) + jnp.dot(scores.astype(jnp.bfloat16), v, preferred_element_type=jnp.float32)
    faded = (k * jnp.exp(jnp.minimum(last - cum, 0.0))).astype(jnp.bfloat16)
    state[...] = held * jnp.exp(last) + lax.dot_general(
        v, faded, (((0,), (0,)), ((), ())), preferred_element_type=jnp.float32
    )
    scale = lax.rsqrt(jnp.mean(readout * readout, axis=-1, keepdims=True) + EPS)
    return (readout * scale * gain).astype(jnp.bfloat16)


def attention_kernel(
    q_ref, k_ref, v_ref, rank_ref, second_ref, bias_ref, surge_ref, gain_ref, o_ref, state
):
    @pl.when(lax.rem(pl.program_id(1), LENGTH // CHUNK) == 0)
    def _():
        state[...] = jnp.zeros_like(state)

    o_ref[...] = attend(
        q_ref[...], k_ref[...], v_ref[...], rank_ref[...], second_ref[...], bias_ref[...],
        surge_ref[0], gain_ref[...], state,
    )


def attention(qkv, rank_rows, second, bias, surge, gain):
    tokens = qkv.shape[0]
    heads = second.shape[1] // KEY_WIDTH
    rank = rank_rows.shape[1]
    value_base = 2 * heads * KEY_WIDTH // DV
    return pl.pallas_call(
        attention_kernel,
        grid=(heads, tokens // CHUNK),
        in_specs=[
            pl.BlockSpec((CHUNK, KEY_WIDTH), lambda h, c: (c, h)),
            pl.BlockSpec((CHUNK, KEY_WIDTH), lambda h, c: (c, heads + h)),
            pl.BlockSpec((CHUNK, DV), lambda h, c: (c, value_base + h)),
            pl.BlockSpec((CHUNK, rank), lambda h, c: (c, 0)),
            pl.BlockSpec((rank, KEY_WIDTH), lambda h, c: (0, h)),
            pl.BlockSpec((1, KEY_WIDTH), lambda h, c: (0, h)),
            pl.BlockSpec((1, CHUNK, 1), lambda h, c: (h, c, 0)),
            pl.BlockSpec((1, DV), lambda h, c: (0, 0)),
        ],
        out_specs=pl.BlockSpec((CHUNK, DV), lambda h, c: (c, h)),
        out_shape=jax.ShapeDtypeStruct((tokens, heads * DV), jnp.bfloat16),
        scratch_shapes=[pltpu.VMEM((DV, KEY_WIDTH), jnp.float32)],
        compiler_params=pltpu.CompilerParams(
            dimension_semantics=("arbitrary", "arbitrary"), vmem_limit_bytes=24 * 2**20
        ),
        cost_estimate=pl.CostEstimate(
            flops=20_000_000_000, bytes_accessed=20_000_000, transcendentals=8_000_000
        ),
        name="attention",
    )(qkv, qkv, qkv, rank_rows, second, bias[None, :], surge.T[:, :, None], gain[None, :])


def on_device(
    n_rep,
    n_fs,
    n_tp,
    tokens,
    attention_pre_gain,
    query_matrix,
    key_matrix,
    value_matrix,
    decay_first_weight,
    decay_second_weight,
    decay_offset_bias,
    extra_log_surge,
    readout_head_gain,
    output_matrix,
    attention_post_gain,
    feedforward_pre_gain,
    up_matrix,
    down_matrix,
    feedforward_post_gain,
):
    me = lax.axis_index("tp")
    rep = lax.axis_index("rep")
    swap = [(i, 1 - i) for i in range(2)]

    def both_halves(mine):
        if n_tp != 2:
            return lax.all_gather(mine, "tp", axis=1, tiled=True)
        other = lax.ppermute(mine, "tp", swap)
        first = me == 0
        return jnp.concatenate(
            [jnp.where(first, mine, other), jnp.where(first, other, mine)], axis=1
        )

    def sum_scattered(partial):
        if n_tp != 2:
            return lax.psum_scatter(partial, "tp", scatter_dimension=1, tiled=True).astype(
                jnp.float32
            )
        size = partial.shape[1] // 2
        keep = lax.dynamic_slice_in_dim(partial, me * size, size, 1)
        send = lax.dynamic_slice_in_dim(partial, (1 - me) * size, size, 1)
        return keep.astype(jnp.float32) + lax.ppermute(send, "tp", swap).astype(jnp.float32)

    def summed(rows):
        if n_tp != 2:
            return lax.psum(rows, "tp")
        return rows + lax.ppermute(rows, "tp", swap)

    def part(weight, axis):
        size = weight.shape[axis] // n_rep
        return lax.dynamic_slice_in_dim(weight, rep * size, size, axis)

    weights = jnp.concatenate([query_matrix, key_matrix, value_matrix], axis=1)
    with jax.named_scope("gather_in"):
        whole_in = lax.all_gather(weights, "fs", axis=0, tiled=True)
    with jax.named_scope("gather_out"):
        whole_out = lax.all_gather(output_matrix, "fs", axis=1, tiled=True)
    rows = up_matrix.shape[0]
    cols = down_matrix.shape[1]
    mine = lax.axis_index("fs")
    place = jnp.where(mine % 2 == 0, mine // 2, n_fs - 1 - mine // 2)
    cycle = [2 * p if p < n_fs // 2 else 2 * (n_fs - 1 - p) + 1 for p in range(n_fs)]
    ahead = [(cycle[p], cycle[(p + 1) % n_fs]) for p in range(n_fs)]
    behind = [(to, at) for at, to in ahead]

    def shard_at(p):
        p = (p + n_fs) % n_fs
        return jnp.where(p < n_fs // 2, 2 * p, 2 * (n_fs - 1 - p) + 1)

    def travel(own, hops_ahead, hops_behind):
        chunks = []
        for hops, ring, sign in ((hops_ahead, ahead, -1), (hops_behind, behind, 1)):
            piece = own
            for step in range(1, hops + 1):
                piece = lax.ppermute(piece, "fs", ring)
                chunks.append((step, shard_at(place + sign * step), piece))
        chunks.sort(key=lambda c: c[0])
        pieces = [(piece, rep, shard) for _, shard, piece in chunks]
        others = []
        for piece, _, shard in pieces:
            for turn in range(1, n_rep):
                other = lax.ppermute(
                    piece, "rep", [(r, (r + turn) % n_rep) for r in range(n_rep)]
                )
                others.append((other, (rep + n_rep - turn) % n_rep, shard))
        return pieces, others

    def hold_until(value, moved):
        tied = lax.optimization_barrier((value, *[m[0] for m in moved]))
        return tied[0], [(t, *m[1:]) for t, m in zip(tied[1:], moved)]

    up_cols = up_matrix.shape[1] // n_rep
    down_rows = down_matrix.shape[0] // n_rep
    half = n_fs // 2
    up_pieces, up_others = travel(part(up_matrix, 1), half, n_fs - 1 - half)
    with jax.named_scope("gather_down"):
        whole_down = lax.all_gather(down_matrix, "fs", axis=1, tiled=True)

    gathered = both_halves(tokens)
    width = gathered.shape[1]
    normed = pre_norm(gathered, attention_pre_gain)
    rank_rows = jnp.dot(normed, decay_first_weight, preferred_element_type=jnp.float32).astype(
        jnp.bfloat16
    )
    early = up_pieces + up_others[: half]
    normed, early = hold_until(normed, early)
    with jax.named_scope("project"):
        qkv = jnp.dot(normed, whole_in, preferred_element_type=jnp.float32).astype(jnp.bfloat16)
    with jax.named_scope("mix"):
        mixed = attention(
            qkv, rank_rows, decay_second_weight, decay_offset_bias, extra_log_surge,
            readout_head_gain,
        )
    mixed, late = hold_until(mixed, up_others[half :])
    with jax.named_scope("out_project"):
        partial_attn = jnp.dot(mixed, whole_out, preferred_element_type=jnp.float32)
    attn = sum_scattered(partial_attn.astype(jnp.bfloat16))
    attn_total = summed(jnp.sum(attn * attn, axis=1))
    attn_scale = lax.rsqrt(attn_total / width + EPS)[:, None]
    resid = (tokens.astype(jnp.float32) + attn * attn_scale * attention_post_gain).astype(
        jnp.bfloat16
    )
    normed_mid = pre_norm(both_halves(resid), feedforward_pre_gain)
    whole_up = lax.dynamic_update_slice(
        jnp.zeros((n_fs * rows, up_matrix.shape[1]), jnp.bfloat16), up_matrix, (mine * rows, 0)
    )
    for piece, r, j in early + late:
        whole_up = lax.dynamic_update_slice(whole_up, piece, (j * rows, r * up_cols))
    hidden = jax.nn.relu(jnp.dot(normed_mid, whole_up, preferred_element_type=jnp.float32))
    squared = (hidden * hidden).astype(jnp.bfloat16)
    partial_feed = jnp.dot(squared, whole_down, preferred_element_type=jnp.float32)
    feed = sum_scattered(partial_feed.astype(jnp.bfloat16))
    feed_total = summed(jnp.sum(feed * feed, axis=1))
    feed_scale = lax.rsqrt(feed_total / width + EPS)[:, None]
    return (resid.astype(jnp.float32) + feed * feed_scale * feedforward_post_gain).astype(
        jnp.bfloat16
    )


MESH = pl.DeviceIdType.MESH
UNIT = 16


def ring_split(rows, heavy_x):
    third = rows / (3 * UNIT)
    a = (math.ceil(third) if heavy_x else math.floor(third)) * UNIT
    return a, rows - 2 * a


def layer_kernel(
    dims,
    tok_hbm,
    pre_gain_hbm,
    wq_hbm,
    wk_hbm,
    wv_hbm,
    first_hbm,
    second_hbm,
    bias_hbm,
    surge_hbm,
    head_gain_hbm,
    out_hbm,
    post_gain_hbm,
    mid_gain_hbm,
    up_hbm,
    down_hbm,
    last_gain_hbm,
    o_hbm,
    wqkv,
    wout,
    wup,
    wdn,
    tok,
    normed,
    rank,
    mixed,
    keep,
    sendb,
    recvb,
    ss,
    ss_in,
    sq,
    fbuf,
    rbuf,
    state,
    pre_gain,
    first_ref,
    second_ref,
    bias_ref,
    surge_ref,
    head_gain,
    post_gain,
    mid_gain,
    last_gain,
    local_sem,
    small_sem,
    put_sem,
    ring_send,
    ring_recv,
    x_send,
    x_recv,
    x_last,
    extra_send,
    extra_recv,
    core_send,
    core_recv,
    feed_send,
    feed_recv,
):
    n_fs = dims["fs"]
    half_ring = n_fs // 2
    rep, fs, tp = lax.axis_index("rep"), lax.axis_index("fs"), lax.axis_index("tp")
    place = jnp.where(lax.rem(fs, 2) == 0, fs // 2, n_fs - 1 - fs // 2)

    def shard_at(p):
        p = lax.rem(p + 2 * n_fs, n_fs)
        return jnp.where(p < half_ring, 2 * p, 2 * (n_fs - 1 - p) + 1)

    ring_id = [{"fs": shard_at(place + 1)}, {"fs": shard_at(place - 1)}]
    x_id = {"rep": 1 - rep}
    core_id = {"tp": 1 - tp}

    tokens, width = normed.shape
    dh = tok.shape[2]
    qkv_rows = wq_hbm.shape[0]
    out_rows = out_hbm.shape[0]
    up_rows = up_hbm.shape[0]
    up_half = up_hbm.shape[1] // 2
    dn_half = down_hbm.shape[0] // 2
    cols = down_hbm.shape[1]
    per_half = n_fs // 2

    def rows_of(ref, shard_rows, lanes):
        def view(j, off, n):
            return ref.at[pl.ds(pl.multiple_of(j * shard_rows + off, UNIT), n), lanes]

        return view

    def slab_of(ref, base):
        def view(j, off, n):
            return ref.at[j, pl.ds(pl.multiple_of(base + off, UNIT), n), :]

        return view

    streams = [
        (rows_of(wqkv, qkv_rows, slice(None)), qkv_rows // 2, ring_split(qkv_rows // 2, True)),
        (slab_of(wout, 0), out_rows // 2, ring_split(out_rows // 2, False)),
        (rows_of(wup, up_rows, slice(0, up_half)), up_rows // 2, ring_split(up_rows // 2, True)),
        (
            rows_of(wup, up_rows, slice(up_half, 2 * up_half)),
            up_rows // 2,
            ring_split(up_rows // 2, False),
        ),
        (slab_of(wdn, 0), dn_half // 2, ring_split(dn_half // 2, True)),
        (slab_of(wdn, dn_half), dn_half // 2, ring_split(dn_half // 2, False)),
    ]
    QKV, OUT, UP0, UP1, DN0, DN1 = range(6)

    def sign(d):
        return 1 - 2 * d

    def chunk_of(e, d):
        return e + d - 2 * e * d

    def ring_copy(s, d, e, h, own_send):
        view, rows, (a, c) = streams[s]
        step = h - 1 if own_send else h
        j = shard_at(place - sign(d) * step)
        piece = view(j, chunk_of(e, d) * rows + rep * a, a + c)
        return pltpu.make_async_remote_copy(
            src_ref=piece,
            dst_ref=piece,
            send_sem=ring_send.at[s],
            recv_sem=ring_recv.at[s % 2, d, e, h - 1],
            device_id=ring_id[d],
            device_id_type=MESH,
        )

    def x_copy(s, d, e, h, own_send):
        view, rows, (a, c) = streams[s]
        j = shard_at(place - sign(d) * h)
        side = rep if own_send else 1 - rep
        piece = view(j, chunk_of(e, d) * rows + side * (a + c), a)
        return pltpu.make_async_remote_copy(
            src_ref=piece,
            dst_ref=piece,
            send_sem=x_send.at[s],
            recv_sem=x_last.at[d, e, h - 1] if s == DN1 else x_recv.at[s],
            device_id=x_id,
            device_id_type=MESH,
        )

    n_items = n_fs - 1

    def begin(s):
        for e in range(2):
            for d in range(2):
                ring_copy(s, d, e, 1, True).start()

    def poll(s, i):
        if isinstance(i, int):
            e, h = i % 2, i // 2 + 1
        else:
            e = lax.rem(i, 2)
            h = i // 2 + 1
        for d in range(2):
            ring_copy(s, d, e, h, False).wait_recv()
            if isinstance(i, int):
                if i + 2 < n_items:
                    ring_copy(s, d, e, h + 1, True).start()
            else:

                @pl.when(i + 2 < n_items)
                def _():
                    ring_copy(s, d, e, h + 1, True).start()

            if s != DN1:
                x_copy(s, d, e, h, True).start()
            else:

                @pl.when(i < n_items - 1)
                def _():
                    x_copy(s, d, e, h, True).start()


    def extra_copy(d, own_send):
        view, rows, (a, c) = streams[DN1]
        step = half_ring - 1 if own_send else half_ring
        j = shard_at(place - sign(d) * step)
        piece = view(j, d * rows + (1 - rep) * (a + c), a)
        return pltpu.make_async_remote_copy(
            src_ref=piece,
            dst_ref=piece,
            send_sem=extra_send.at[d],
            recv_sem=extra_recv.at[d],
            device_id=ring_id[d],
            device_id_type=MESH,
        )

    def all_bytes(s, rows, sem, count=2 * n_items):
        ref, lanes = [
            (wqkv, wqkv.shape[1]),
            (wout, None),
            (wup, up_half),
            (wup, up_half),
            (wdn, None),
            (wdn, None),
        ][s]
        if lanes is None:
            half = count // 2
            whole = ref.at[0:half, 0 : 2 * rows, :]
        else:
            whole = ref.at[0 : count * rows, 0:lanes]
        return pltpu.make_async_copy(whole, whole, sem)

    def x_wait(s):
        all_bytes(s, streams[s][2][0], x_recv.at[s]).wait()

    head_cols = wq_hbm.shape[1]
    own = [
        pltpu.make_async_copy(
            wq_hbm,
            wqkv.at[pl.ds(pl.multiple_of(fs * qkv_rows, UNIT), qkv_rows), 0:head_cols],
            local_sem.at[0],
        ),
        pltpu.make_async_copy(
            wk_hbm,
            wqkv.at[
                pl.ds(pl.multiple_of(fs * qkv_rows, UNIT), qkv_rows), head_cols : 2 * head_cols
            ],
            local_sem.at[1],
        ),
        pltpu.make_async_copy(
            wv_hbm,
            wqkv.at[pl.ds(pl.multiple_of(fs * qkv_rows, UNIT), qkv_rows), 2 * head_cols :],
            local_sem.at[2],
        ),
        pltpu.make_async_copy(tok_hbm, tok.at[tp], local_sem.at[3]),
        pltpu.make_async_copy(out_hbm, wout.at[fs], local_sem.at[4]),
        pltpu.make_async_copy(
            up_hbm,
            wup.at[pl.ds(pl.multiple_of(fs * up_rows, UNIT), up_rows), :],
            local_sem.at[5],
        ),
        pltpu.make_async_copy(down_hbm, wdn.at[fs], local_sem.at[6]),
    ]
    small = [
        pltpu.make_async_copy(src, dst, small_sem.at[n])
        for n, (src, dst) in enumerate(
            (
                (pre_gain_hbm, pre_gain),
                (first_hbm, first_ref),
                (second_hbm, second_ref),
                (bias_hbm, bias_ref),
                (surge_hbm, surge_ref),
                (head_gain_hbm, head_gain),
                (post_gain_hbm, post_gain),
                (mid_gain_hbm, mid_gain),
                (last_gain_hbm, last_gain),
            )
        )
    ]
    for copy in (*own[:4], *small, *own[4:]):
        copy.start()

    barrier = pltpu.get_barrier_semaphore()
    for target in (*ring_id, x_id, core_id):
        pl.semaphore_signal(barrier, inc=1, device_id=target, device_id_type=MESH)
    pl.semaphore_wait(barrier, 4)

    for copy in own[:3]:
        copy.wait()
    begin(QKV)

    def core_copy(k, src, dst):
        return pltpu.make_async_remote_copy(
            src_ref=src,
            dst_ref=dst,
            send_sem=core_send.at[k],
            recv_sem=core_recv.at[k],
            device_id=core_id,
            device_id_type=MESH,
        )

    own[3].wait()
    swap_tok = core_copy(0, tok.at[tp], tok.at[tp])
    swap_tok.start()
    for copy in (*small, *own[4:]):
        copy.wait()
    core_copy(0, tok.at[1 - tp], tok.at[1 - tp]).wait_recv()

    def norm_rows(gain, count, part=0, parts=1):
        def body(r, carry):
            at = pl.ds(pl.multiple_of(r * count, count), count)
            left = tok[0, at, :].astype(jnp.float32)
            right = tok[1, at, :].astype(jnp.float32)
            total = jnp.sum(left * left, axis=1, keepdims=True) + jnp.sum(
                right * right, axis=1, keepdims=True
            )
            scale = lax.rsqrt(total / width + EPS)
            normed[at, 0:dh] = (left * scale * gain[:, 0:dh]).astype(jnp.bfloat16)
            normed[at, dh:] = (right * scale * gain[:, dh:]).astype(jnp.bfloat16)
            return carry

        span = tokens // count // parts
        lax.fori_loop(part * span, (part + 1) * span, body, 0)

    norm_rows(pre_gain, 64)
    poll(QKV, 0)

    def rank_body(r, carry):
        at = pl.ds(pl.multiple_of(r * 256, 256), 256)
        rank[at, :] = lax.dot_general(
            normed[at, :],
            first_ref[...],
            (((1,), (1,)), ((), ())),
            preferred_element_type=jnp.float32,
        ).astype(jnp.bfloat16)
        return carry

    lax.fori_loop(0, tokens // 256, rank_body, 0)
    for i in range(1, n_items):
        poll(QKV, i)
        if i == n_items - 3:
            begin(OUT)

    for i in range(n_items):
        poll(OUT, i)
        if i == n_items - 3:
            begin(UP0)
    x_wait(QKV)

    chunks = tokens // CHUNK

    def attention_chunk(chunk, carry):
        @pl.when(chunk < n_items)
        def _():
            poll(UP0, chunk)

        @pl.when(chunk == n_items - 3)
        def _():
            begin(UP1)

        @pl.when(lax.rem(chunk, LENGTH // CHUNK) == 0)
        def _():
            state[...] = jnp.zeros_like(state)

        at = pl.ds(pl.multiple_of(chunk * CHUNK, CHUNK), CHUNK)
        surge_row = surge_ref[:, pl.ds(pl.multiple_of(chunk * CHUNK, CHUNK), CHUNK)]
        surge = jnp.transpose(jnp.broadcast_to(surge_row, (8, CHUNK)))[:, 0:1]
        qkv = jnp.dot(
            normed[at, :], wqkv[...], preferred_element_type=jnp.float32
        ).astype(jnp.bfloat16)
        mixed[at, :] = attend(
            qkv[:, 0:head_cols],
            qkv[:, head_cols : 2 * head_cols],
            qkv[:, 2 * head_cols :],
            rank[at, :],
            second_ref[...],
            bias_ref[...],
            surge,
            head_gain[...],
            state,
        )
        return carry

    lax.fori_loop(0, chunks, attention_chunk, 0)

    poll(UP1, 0)
    x_wait(OUT)

    def out_rows_body(r, carry):
        at = pl.ds(pl.multiple_of(r * 256, 256), 256)
        rows = mixed[at, :]
        for k in range(per_half):
            keep[at, k * cols : (k + 1) * cols] = jnp.dot(
                rows, wout[tp * per_half + k], preferred_element_type=jnp.float32
            ).astype(jnp.bfloat16)
            sendb[at, k * cols : (k + 1) * cols] = jnp.dot(
                rows, wout[(1 - tp) * per_half + k], preferred_element_type=jnp.float32
            ).astype(jnp.bfloat16)
        return carry

    row_blocks = tokens // 256
    lax.fori_loop(0, row_blocks // 2, out_rows_body, 0)
    poll(UP1, 1)
    lax.fori_loop(row_blocks // 2, row_blocks, out_rows_body, 0)
    core_copy(1, sendb, recvb).start()
    poll(UP1, 2)
    core_copy(1, sendb, recvb).wait_recv()

    def attn_rows(r, count):
        at = pl.ds(pl.multiple_of(r * count, count), count)
        return at, keep[at, :].astype(jnp.float32) + recvb[at, :].astype(jnp.float32)

    def square_body(r, carry):
        at, attn = attn_rows(r, 64)
        ss[at, :] = jnp.broadcast_to(
            jnp.sum(attn * attn, axis=1, keepdims=True), (64, ss.shape[1])
        )
        return carry

    lax.fori_loop(0, tokens // 64, square_body, 0)
    core_copy(2, ss, ss_in).start()
    poll(UP1, 3)
    core_copy(2, ss, ss_in).wait_recv()

    def resid_body(r, carry):
        at, attn = attn_rows(r, 64)
        total = ss[at, 0:1] + ss_in[at, 0:1]
        scale = lax.rsqrt(total / width + EPS)
        tok[tp, at, :] = (
            tok[tp, at, :].astype(jnp.float32) + attn * scale * post_gain[...]
        ).astype(jnp.bfloat16)
        return carry

    swap_tok.wait_send()
    lax.fori_loop(0, tokens // 64, resid_body, 0)
    swap_resid = core_copy(3, tok.at[tp], tok.at[tp])
    swap_resid.start()
    poll(UP1, 4)
    begin(DN0)
    core_copy(3, tok.at[1 - tp], tok.at[1 - tp]).wait_recv()
    norm_rows(mid_gain, 64, 0, 2)
    poll(UP1, 5)
    norm_rows(mid_gain, 64, 1, 2)
    poll(UP1, 6)

    blocks = 8
    hidden_cols = wup.shape[1] // blocks

    def up_body(b, carry):
        @pl.when(b < n_items)
        def _():
            poll(DN0, b)

        @pl.when(b == n_items - 3)
        def _():
            begin(DN1)

        @pl.when(b == 1)
        def _():
            x_wait(UP0)
            x_wait(UP1)

        @pl.when(b >= 1)
        def _():
            lanes = pl.ds(pl.multiple_of((b - 1) * hidden_cols, hidden_cols), hidden_cols)
            for r in range(tokens // 256):
                at = slice(r * 256, (r + 1) * 256)
                hidden = jnp.maximum(
                    jnp.dot(normed[at, :], wup[:, lanes], preferred_element_type=jnp.float32),
                    0.0,
                )
                sq[at, lanes] = (hidden * hidden).astype(jnp.bfloat16)

        return carry

    lax.fori_loop(0, blocks + 1, up_body, 0)

    def feed_copy(t):
        j, _, _ = shard_of(t)
        return pltpu.make_async_remote_copy(
            src_ref=fbuf.at[j],
            dst_ref=rbuf.at[j],
            send_sem=feed_send.at[t],
            recv_sem=feed_recv.at[t],
            device_id=core_id,
            device_id_type=MESH,
        )

    def shard_of(t):
        h = (t + 1) // 2
        d = 1 - lax.rem(t, 2)
        return shard_at(place - sign(d) * h), d, h

    def down_of(t):
        j, _, _ = shard_of(t)

        def body(r, carry):
            at = pl.ds(pl.multiple_of(r * 512, 512), 512)
            fbuf[j, at, :] = jnp.dot(
                sq[at, :], wdn[j], preferred_element_type=jnp.float32
            ).astype(jnp.bfloat16)
            return carry

        lax.fori_loop(0, tokens // 512, body, 0)

    def feed_rows(j, at):
        return fbuf[j, at, :].astype(jnp.float32) + rbuf[j, at, :].astype(jnp.float32)

    def squares_of(t):
        j, _, _ = shard_of(t)
        feed_copy(t).wait_recv()

        def body(r, carry):
            at = pl.ds(pl.multiple_of(r * 64, 64), 64)
            feed = feed_rows(j, at)
            ss[at, :] += jnp.broadcast_to(
                jnp.sum(feed * feed, axis=1, keepdims=True), (64, ss.shape[1])
            )
            return carry

        lax.fori_loop(0, tokens // 64, body, 0)

    def last_x(d, e, h):
        x_copy(DN1, d, e, h, False).wait_recv()

    far = half_ring - 1

    def down_body(i, carry):
        poll(DN1, i)

        @pl.when(i == 2)
        def _():
            x_wait(DN0)

        @pl.when((i >= 2) & (i < n_items - 1))
        def _():
            _, d, h = shard_of(i - 1)
            last_x(d, 0, h)
            last_x(d, 1, h)

        @pl.when(i == n_items - 1)
        def _():
            last_x(0, 1, far)

        @pl.when(i != 1)
        def _():
            down_of(jnp.maximum(i - 1, 0))

        @pl.when(i == n_items - 2)
        def _():
            for d in range(2):
                last_x(d, 0, far)
                extra_copy(d, True).start()

        @pl.when((i == 1) | (i >= 3))
        def _():
            feed_copy(jnp.maximum(i - 2, 0)).start()

        @pl.when(i >= 3)
        def _():
            squares_of(i - 3)

        return carry

    core_copy(2, ss, ss_in).wait_send()
    ss[...] = jnp.zeros_like(ss)
    lax.fori_loop(0, n_items, down_body, 0)
    feed_copy(n_fs - 3).start()
    squares_of(n_fs - 4)
    last_x(1, 1, far)
    down_of(n_fs - 2)
    squares_of(n_fs - 3)
    feed_copy(n_fs - 2).start()
    for d in range(2):
        extra_copy(d, False).wait_recv()
    down_of(n_fs - 1)
    feed_copy(n_fs - 1).start()
    squares_of(n_fs - 2)
    squares_of(n_fs - 1)
    core_copy(1, sendb, recvb).wait_send()

    def put_rows(r):
        at = pl.ds(pl.multiple_of(r * 128, 128), 128)
        return pltpu.make_async_copy(sendb.at[at, :], o_hbm.at[at, :], put_sem.at[r])

    def last_body(r, carry):
        at = pl.ds(pl.multiple_of(r * 128, 128), 128)
        scale = lax.rsqrt(ss[at, 0:1] / width + EPS)
        for k in range(per_half):
            lanes = slice(k * cols, (k + 1) * cols)
            feed = feed_rows(tp * per_half + k, at)
            sendb[at, lanes] = (
                tok[tp, at, lanes].astype(jnp.float32) + feed * scale * last_gain[:, lanes]
            ).astype(jnp.bfloat16)

        @pl.when(r >= 1)
        def _():
            put_rows(jnp.maximum(r - 1, 0)).start()

        return carry

    lax.fori_loop(0, tokens // 128, last_body, 0)
    put_rows(tokens // 128 - 1).start()

    for s in range(len(streams)):
        a, c = streams[s][2]
        all_bytes(s, a + c, ring_send.at[s]).wait()
        all_bytes(s, a, x_send.at[s], 2 * n_items - 2 * (s == DN1)).wait()
    for d in range(2):
        extra_copy(d, True).wait_send()
    swap_resid.wait_send()
    for t in range(n_fs):
        feed_copy(t).wait_send()
    for r in range(tokens // 128):
        put_rows(r).wait()


def fused_layer(
    n_rep,
    n_fs,
    n_tp,
    tokens,
    attention_pre_gain,
    query_matrix,
    key_matrix,
    value_matrix,
    decay_first_weight,
    decay_second_weight,
    decay_offset_bias,
    extra_log_surge,
    readout_head_gain,
    output_matrix,
    attention_post_gain,
    feedforward_pre_gain,
    up_matrix,
    down_matrix,
    feedforward_post_gain,
):
    rows, dh = tokens.shape
    width = dh * n_tp
    qkv_cols = query_matrix.shape[1] + key_matrix.shape[1] + value_matrix.shape[1]
    hidden = up_matrix.shape[1]
    cols = down_matrix.shape[1]
    bf = jnp.bfloat16
    any_spec = pl.BlockSpec(memory_space=pl.ANY)
    dma = pltpu.SemaphoreType.DMA
    small = (
        attention_pre_gain[None, :],
        decay_first_weight.T,
        decay_second_weight,
        decay_offset_bias[None, :],
        extra_log_surge.T,
        readout_head_gain[None, :],
        attention_post_gain[None, :],
        feedforward_pre_gain[None, :],
        feedforward_post_gain[None, :],
    )
    return pl.pallas_call(
        functools.partial(layer_kernel, {"fs": n_fs}),
        out_shape=jax.ShapeDtypeStruct((rows, dh), bf),
        in_specs=[any_spec] * 16,
        out_specs=any_spec,
        scratch_shapes=[
            pltpu.VMEM((width, qkv_cols), bf),
            pltpu.VMEM((n_fs, output_matrix.shape[0], cols), bf),
            pltpu.VMEM((width, hidden), bf),
            pltpu.VMEM((n_fs, hidden, cols), bf),
            pltpu.VMEM((n_tp, rows, dh), bf),
            pltpu.VMEM((rows, width), bf),
            pltpu.VMEM((rows, decay_first_weight.shape[1]), bf),
            pltpu.VMEM((rows, DV), bf),
            pltpu.VMEM((rows, dh), bf),
            pltpu.VMEM((rows, dh), bf),
            pltpu.VMEM((rows, dh), bf),
            pltpu.VMEM((rows, 128), jnp.float32),
            pltpu.VMEM((rows, 128), jnp.float32),
            pltpu.VMEM((rows, hidden), bf),
            pltpu.VMEM((n_fs, rows, cols), bf),
            pltpu.VMEM((n_fs, rows, cols), bf),
            pltpu.VMEM((DV, KEY_WIDTH), jnp.float32),
            *[pltpu.VMEM(a.shape, a.dtype) for a in small],
            dma((7,)),
            dma((len(small),)),
            dma((rows // 128,)),
            dma((6,)),
            dma((2, 2, 2, n_fs // 2)),
            dma((6,)),
            dma((5,)),
            dma((2, 2, n_fs // 2)),
            dma((2,)),
            dma((2,)),
            dma((4,)),
            dma((4,)),
            dma((n_fs,)),
            dma((n_fs,)),
        ],
        compiler_params=pltpu.CompilerParams(
            collective_id=0, has_side_effects=True, vmem_limit_bytes=60 * 2**20
        ),
        name="layer",
    )(
        tokens,
        small[0],
        query_matrix,
        key_matrix,
        value_matrix,
        *small[1:6],
        output_matrix,
        *small[6:8],
        up_matrix,
        down_matrix,
        small[8],
    )


def per_device(n_rep, n_fs, n_tp, *args):
    tokens, query, second, out, up, down = args[0], args[2], args[6], args[10], args[13], args[14]
    fits = (
        n_rep == 2
        and n_tp == 2
        and n_fs % 2 == 0
        and 6 <= n_fs <= 8
        and tokens.shape[0] % LENGTH == 0
        and tokens.shape[0] // CHUNK == n_fs
        and second.shape[1] == KEY_WIDTH
        and out.shape[1] % 128 == 0
        and query.shape[0] % (8 * UNIT) == 0
        and up.shape[0] % (8 * UNIT) == 0
        and down.shape[1] == out.shape[1]
    )
    return (fused_layer if fits else on_device)(n_rep, n_fs, n_tp, *args)


def solution(mesh):
    return jax.shard_map(
        functools.partial(per_device, mesh.shape["rep"], mesh.shape["fs"], mesh.shape["tp"]),
        mesh=mesh,
        in_specs=(
            P(("rep", "fs"), "tp"),
            P(),
            P("fs", "tp"),
            P("fs", "tp"),
            P("fs", "tp"),
            P(),
            P(None, "tp"),
            P("tp"),
            P(("rep", "fs"), "tp"),
            P(),
            P("tp", "fs"),
            P("tp"),
            P(),
            P("fs", "tp"),
            P("tp", "fs"),
            P("tp"),
        ),
        out_specs=P(("rep", "fs"), "tp"),
        check_vma=False,
    )
```

```python
import functools
import math

import jax
import jax.numpy as jnp
from jax import lax
from jax.experimental import pallas as pl
from jax.experimental.pallas import tpu as pltpu
from jax.sharding import PartitionSpec as P

KEY_WIDTH = 256
DV = 512
LENGTH = 1024
CHUNK = 128
SUB = 16
EPS = 1e-06


def pre_norm(rows, gain):
    values = rows.astype(jnp.float32)
    scale = lax.rsqrt(jnp.mean(values * values, axis=-1, keepdims=True) + EPS)
    return (values * scale * gain).astype(jnp.bfloat16)


def attend(q, k, v, rank_rows, second, bias, surge, gain, state):
    subs = CHUNK // SUB
    q = q.astype(jnp.float32) * KEY_WIDTH ** (-0.5)
    k = k.astype(jnp.float32)
    source = jnp.dot(rank_rows, second, preferred_element_type=jnp.float32) + bias
    log_sig = jnp.minimum(source, 0.0) - jnp.log1p(jnp.exp(-jnp.abs(source)))
    gate = log_sig / 16.0 + surge

    row = lax.broadcasted_iota(jnp.int32, (CHUNK, CHUNK), 0)
    col = lax.broadcasted_iota(jnp.int32, (CHUNK, CHUNK), 1)
    lower = (row >= col).astype(jnp.float32)
    cum = jnp.dot(
        lower, gate, preferred_element_type=jnp.float32, precision=lax.Precision.HIGHEST
    )

    q3 = q.reshape(subs, SUB, KEY_WIDTH)
    k3 = k.reshape(subs, SUB, KEY_WIDTH)
    c3 = cum.reshape(subs, SUB, KEY_WIDTH)
    pick_col = lax.rem(lax.broadcasted_iota(jnp.int32, (KEY_WIDTH, CHUNK), 1), SUB)
    scores = jnp.zeros((CHUNK, CHUNK), jnp.float32)
    for j in range(SUB):
        weight = jnp.exp(jnp.minimum(c3 - c3[:, j : j + 1, :], 0.0))
        term = (q3 * k3[:, j : j + 1, :] * weight).reshape(CHUNK, KEY_WIDTH)
        scores += jnp.dot(
            term.astype(jnp.bfloat16),
            (pick_col == j).astype(jnp.bfloat16),
            preferred_element_type=jnp.float32,
        )
    scores = jnp.where((row // SUB == col // SUB) & (row >= col), scores, 0.0)

    pieces = [jnp.zeros((SUB, CHUNK), jnp.float32)]
    key_row = lax.broadcasted_iota(jnp.int32, (CHUNK, KEY_WIDTH), 0)
    for i in range(1, subs):
        edge = cum[i * SUB - 1 : i * SUB, :]
        left = q3[i] * jnp.exp(jnp.minimum(c3[i] - edge, 0.0))
        right = jnp.where(key_row < i * SUB, k * jnp.exp(jnp.minimum(edge - cum, 0.0)), 0.0)
        pieces.append(
            lax.dot_general(
                left.astype(jnp.bfloat16),
                right.astype(jnp.bfloat16),
                (((1,), (1,)), ((), ())),
                preferred_element_type=jnp.float32,
            )
        )
    scores = scores + jnp.concatenate(pieces, axis=0)

    last = cum[CHUNK - 1 : CHUNK, :]
    held = state[...]
    readout = lax.dot_general(
        (q * jnp.exp(cum)).astype(jnp.bfloat16),
        held.astype(jnp.bfloat16),
        (((1,), (1,)), ((), ())),
        preferred_element_type=jnp.float32,
    ) + jnp.dot(scores.astype(jnp.bfloat16), v, preferred_element_type=jnp.float32)
    faded = (k * jnp.exp(jnp.minimum(last - cum, 0.0))).astype(jnp.bfloat16)
    state[...] = held * jnp.exp(last) + lax.dot_general(
        v, faded, (((0,), (0,)), ((), ())), preferred_element_type=jnp.float32
    )
    scale = lax.rsqrt(jnp.mean(readout * readout, axis=-1, keepdims=True) + EPS)
    return (readout * scale * gain).astype(jnp.bfloat16)


def attention_kernel(
    q_ref, k_ref, v_ref, rank_ref, second_ref, bias_ref, surge_ref, gain_ref, o_ref, state
):
    @pl.when(lax.rem(pl.program_id(1), LENGTH // CHUNK) == 0)
    def _():
        state[...] = jnp.zeros_like(state)

    o_ref[...] = attend(
        q_ref[...], k_ref[...], v_ref[...], rank_ref[...], second_ref[...], bias_ref[...],
        surge_ref[0], gain_ref[...], state,
    )


def attention(qkv, rank_rows, second, bias, surge, gain):
    tokens = qkv.shape[0]
    heads = second.shape[1] // KEY_WIDTH
    rank = rank_rows.shape[1]
    value_base = 2 * heads * KEY_WIDTH // DV
    return pl.pallas_call(
        attention_kernel,
        grid=(heads, tokens // CHUNK),
        in_specs=[
            pl.BlockSpec((CHUNK, KEY_WIDTH), lambda h, c: (c, h)),
            pl.BlockSpec((CHUNK, KEY_WIDTH), lambda h, c: (c, heads + h)),
            pl.BlockSpec((CHUNK, DV), lambda h, c: (c, value_base + h)),
            pl.BlockSpec((CHUNK, rank), lambda h, c: (c, 0)),
            pl.BlockSpec((rank, KEY_WIDTH), lambda h, c: (0, h)),
            pl.BlockSpec((1, KEY_WIDTH), lambda h, c: (0, h)),
            pl.BlockSpec((1, CHUNK, 1), lambda h, c: (h, c, 0)),
            pl.BlockSpec((1, DV), lambda h, c: (0, 0)),
        ],
        out_specs=pl.BlockSpec((CHUNK, DV), lambda h, c: (c, h)),
        out_shape=jax.ShapeDtypeStruct((tokens, heads * DV), jnp.bfloat16),
        scratch_shapes=[pltpu.VMEM((DV, KEY_WIDTH), jnp.float32)],
        compiler_params=pltpu.CompilerParams(
            dimension_semantics=("arbitrary", "arbitrary"), vmem_limit_bytes=24 * 2**20
        ),
        cost_estimate=pl.CostEstimate(
            flops=20_000_000_000, bytes_accessed=20_000_000, transcendentals=8_000_000
        ),
        name="attention",
    )(qkv, qkv, qkv, rank_rows, second, bias[None, :], surge.T[:, :, None], gain[None, :])


def on_device(
    n_rep,
    n_fs,
    n_tp,
    tokens,
    attention_pre_gain,
    query_matrix,
    key_matrix,
    value_matrix,
    decay_first_weight,
    decay_second_weight,
    decay_offset_bias,
    extra_log_surge,
    readout_head_gain,
    output_matrix,
    attention_post_gain,
    feedforward_pre_gain,
    up_matrix,
    down_matrix,
    feedforward_post_gain,
):
    me = lax.axis_index("tp")
    rep = lax.axis_index("rep")
    swap = [(i, 1 - i) for i in range(2)]

    def both_halves(mine):
        if n_tp != 2:
            return lax.all_gather(mine, "tp", axis=1, tiled=True)
        other = lax.ppermute(mine, "tp", swap)
        first = me == 0
        return jnp.concatenate(
            [jnp.where(first, mine, other), jnp.where(first, other, mine)], axis=1
        )

    def sum_scattered(partial):
        if n_tp != 2:
            return lax.psum_scatter(partial, "tp", scatter_dimension=1, tiled=True).astype(
                jnp.float32
            )
        size = partial.shape[1] // 2
        keep = lax.dynamic_slice_in_dim(partial, me * size, size, 1)
        send = lax.dynamic_slice_in_dim(partial, (1 - me) * size, size, 1)
        return keep.astype(jnp.float32) + lax.ppermute(send, "tp", swap).astype(jnp.float32)

    def summed(rows):
        if n_tp != 2:
            return lax.psum(rows, "tp")
        return rows + lax.ppermute(rows, "tp", swap)

    def part(weight, axis):
        size = weight.shape[axis] // n_rep
        return lax.dynamic_slice_in_dim(weight, rep * size, size, axis)

    weights = jnp.concatenate([query_matrix, key_matrix, value_matrix], axis=1)
    with jax.named_scope("gather_in"):
        whole_in = lax.all_gather(weights, "fs", axis=0, tiled=True)
    with jax.named_scope("gather_out"):
        whole_out = lax.all_gather(output_matrix, "fs", axis=1, tiled=True)
    rows = up_matrix.shape[0]
    cols = down_matrix.shape[1]
    mine = lax.axis_index("fs")
    place = jnp.where(mine % 2 == 0, mine // 2, n_fs - 1 - mine // 2)
    cycle = [2 * p if p < n_fs // 2 else 2 * (n_fs - 1 - p) + 1 for p in range(n_fs)]
    ahead = [(cycle[p], cycle[(p + 1) % n_fs]) for p in range(n_fs)]
    behind = [(to, at) for at, to in ahead]

    def shard_at(p):
        p = (p + n_fs) % n_fs
        return jnp.where(p < n_fs // 2, 2 * p, 2 * (n_fs - 1 - p) + 1)

    def travel(own, hops_ahead, hops_behind):
        chunks = []
        for hops, ring, sign in ((hops_ahead, ahead, -1), (hops_behind, behind, 1)):
            piece = own
            for step in range(1, hops + 1):
                piece = lax.ppermute(piece, "fs", ring)
                chunks.append((step, shard_at(place + sign * step), piece))
        chunks.sort(key=lambda c: c[0])
        pieces = [(piece, rep, shard) for _, shard, piece in chunks]
        others = []
        for piece, _, shard in pieces:
            for turn in range(1, n_rep):
                other = lax.ppermute(
                    piece, "rep", [(r, (r + turn) % n_rep) for r in range(n_rep)]
                )
                others.append((other, (rep + n_rep - turn) % n_rep, shard))
        return pieces, others

    def hold_until(value, moved):
        tied = lax.optimization_barrier((value, *[m[0] for m in moved]))
        return tied[0], [(t, *m[1:]) for t, m in zip(tied[1:], moved)]

    up_cols = up_matrix.shape[1] // n_rep
    down_rows = down_matrix.shape[0] // n_rep
    half = n_fs // 2
    up_pieces, up_others = travel(part(up_matrix, 1), half, n_fs - 1 - half)
    with jax.named_scope("gather_down"):
        whole_down = lax.all_gather(down_matrix, "fs", axis=1, tiled=True)

    gathered = both_halves(tokens)
    width = gathered.shape[1]
    normed = pre_norm(gathered, attention_pre_gain)
    rank_rows = jnp.dot(normed, decay_first_weight, preferred_element_type=jnp.float32).astype(
        jnp.bfloat16
    )
    early = up_pieces + up_others[: half]
    normed, early = hold_until(normed, early)
    with jax.named_scope("project"):
        qkv = jnp.dot(normed, whole_in, preferred_element_type=jnp.float32).astype(jnp.bfloat16)
    with jax.named_scope("mix"):
        mixed = attention(
            qkv, rank_rows, decay_second_weight, decay_offset_bias, extra_log_surge,
            readout_head_gain,
        )
    mixed, late = hold_until(mixed, up_others[half :])
    with jax.named_scope("out_project"):
        partial_attn = jnp.dot(mixed, whole_out, preferred_element_type=jnp.float32)
    attn = sum_scattered(partial_attn.astype(jnp.bfloat16))
    attn_total = summed(jnp.sum(attn * attn, axis=1))
    attn_scale = lax.rsqrt(attn_total / width + EPS)[:, None]
    resid = (tokens.astype(jnp.float32) + attn * attn_scale * attention_post_gain).astype(
        jnp.bfloat16
    )
    normed_mid = pre_norm(both_halves(resid), feedforward_pre_gain)
    whole_up = lax.dynamic_update_slice(
        jnp.zeros((n_fs * rows, up_matrix.shape[1]), jnp.bfloat16), up_matrix, (mine * rows, 0)
    )
    for piece, r, j in early + late:
        whole_up = lax.dynamic_update_slice(whole_up, piece, (j * rows, r * up_cols))
    hidden = jax.nn.relu(jnp.dot(normed_mid, whole_up, preferred_element_type=jnp.float32))
    squared = (hidden * hidden).astype(jnp.bfloat16)
    partial_feed = jnp.dot(squared, whole_down, preferred_element_type=jnp.float32)
    feed = sum_scattered(partial_feed.astype(jnp.bfloat16))
    feed_total = summed(jnp.sum(feed * feed, axis=1))
    feed_scale = lax.rsqrt(feed_total / width + EPS)[:, None]
    return (resid.astype(jnp.float32) + feed * feed_scale * feedforward_post_gain).astype(
        jnp.bfloat16
    )


MESH = pl.DeviceIdType.MESH
UNIT = 16
LAST_BLOCKS = 2


def ring_split(rows, heavy_x):
    third = rows / (3 * UNIT)
    a = (math.ceil(third) if heavy_x else math.floor(third)) * UNIT
    return a, rows - 2 * a


def layer_kernel(
    dims,
    tok_hbm,
    pre_gain_hbm,
    wq_hbm,
    wk_hbm,
    wv_hbm,
    first_hbm,
    second_hbm,
    bias_hbm,
    surge_hbm,
    head_gain_hbm,
    out_hbm,
    post_gain_hbm,
    mid_gain_hbm,
    up_hbm,
    down_hbm,
    last_gain_hbm,
    o_ref,
    wqkv,
    wout,
    wup,
    wdn,
    tok,
    normed,
    rank,
    mixed,
    keep,
    sendb,
    recvb,
    ss,
    ss_in,
    sq,
    fbuf,
    rbuf,
    state,
    pre_gain,
    first_ref,
    second_ref,
    bias_ref,
    surge_ref,
    head_gain,
    post_gain,
    mid_gain,
    last_gain,
    local_sem,
    small_sem,
    last_send,
    last_recv,
    ring_send,
    ring_recv,
    x_send,
    x_recv,
    x_last,
    extra_send,
    extra_recv,
    core_send,
    core_recv,
    feed_send,
    feed_recv,
):
    n_fs = dims["fs"]
    half_ring = n_fs // 2
    rep, fs, tp = lax.axis_index("rep"), lax.axis_index("fs"), lax.axis_index("tp")
    place = jnp.where(lax.rem(fs, 2) == 0, fs // 2, n_fs - 1 - fs // 2)

    def shard_at(p):
        p = lax.rem(p + 2 * n_fs, n_fs)
        return jnp.where(p < half_ring, 2 * p, 2 * (n_fs - 1 - p) + 1)

    ring_id = [{"fs": shard_at(place + 1)}, {"fs": shard_at(place - 1)}]
    x_id = {"rep": 1 - rep}
    core_id = {"tp": 1 - tp}

    tokens, width = normed.shape
    dh = tok.shape[2]
    qkv_rows = wq_hbm.shape[0]
    out_rows = out_hbm.shape[0]
    up_rows = up_hbm.shape[0]
    up_half = up_hbm.shape[1] // 2
    dn_half = down_hbm.shape[0] // 2
    cols = down_hbm.shape[1]
    per_half = n_fs // 2

    def rows_of(ref, shard_rows, lanes):
        def view(j, off, n):
            return ref.at[pl.ds(pl.multiple_of(j * shard_rows + off, UNIT), n), lanes]

        return view

    def slab_of(ref, base):
        def view(j, off, n):
            return ref.at[j, pl.ds(pl.multiple_of(base + off, UNIT), n), :]

        return view

    streams = [
        (rows_of(wqkv, qkv_rows, slice(None)), qkv_rows // 2, ring_split(qkv_rows // 2, True)),
        (slab_of(wout, 0), out_rows // 2, ring_split(out_rows // 2, False)),
        (rows_of(wup, up_rows, slice(0, up_half)), up_rows // 2, ring_split(up_rows // 2, True)),
        (
            rows_of(wup, up_rows, slice(up_half, 2 * up_half)),
            up_rows // 2,
            ring_split(up_rows // 2, False),
        ),
        (slab_of(wdn, 0), dn_half // 2, ring_split(dn_half // 2, True)),
        (slab_of(wdn, dn_half), dn_half // 2, ring_split(dn_half // 2, False)),
    ]
    QKV, OUT, UP0, UP1, DN0, DN1 = range(6)

    def sign(d):
        return 1 - 2 * d

    def chunk_of(e, d):
        return e + d - 2 * e * d

    def ring_copy(s, d, e, h, own_send):
        view, rows, (a, c) = streams[s]
        step = h - 1 if own_send else h
        j = shard_at(place - sign(d) * step)
        piece = view(j, chunk_of(e, d) * rows + rep * a, a + c)
        return pltpu.make_async_remote_copy(
            src_ref=piece,
            dst_ref=piece,
            send_sem=ring_send.at[s],
            recv_sem=ring_recv.at[s % 2, d, e, h - 1],
            device_id=ring_id[d],
            device_id_type=MESH,
        )

    def x_copy(s, d, e, h, own_send):
        view, rows, (a, c) = streams[s]
        j = shard_at(place - sign(d) * h)
        side = rep if own_send else 1 - rep
        piece = view(j, chunk_of(e, d) * rows + side * (a + c), a)
        return pltpu.make_async_remote_copy(
            src_ref=piece,
            dst_ref=piece,
            send_sem=x_send.at[s],
            recv_sem=x_last.at[d, e, h - 1] if s == DN1 else x_recv.at[s],
            device_id=x_id,
            device_id_type=MESH,
        )

    n_items = n_fs - 1

    def begin(s):
        for e in range(2):
            for d in range(2):
                ring_copy(s, d, e, 1, True).start()

    def poll(s, i):
        if isinstance(i, int):
            e, h = i % 2, i // 2 + 1
        else:
            e = lax.rem(i, 2)
            h = i // 2 + 1
        for d in range(2):
            ring_copy(s, d, e, h, False).wait_recv()
            if isinstance(i, int):
                if i + 2 < n_items:
                    ring_copy(s, d, e, h + 1, True).start()
            else:

                @pl.when(i + 2 < n_items)
                def _():
                    ring_copy(s, d, e, h + 1, True).start()

            if s != DN1:
                x_copy(s, d, e, h, True).start()
            else:

                @pl.when(i < n_items - 1)
                def _():
                    x_copy(s, d, e, h, True).start()


    def extra_copy(d, own_send):
        view, rows, (a, c) = streams[DN1]
        step = half_ring - 1 if own_send else half_ring
        j = shard_at(place - sign(d) * step)
        piece = view(j, d * rows + (1 - rep) * (a + c), a)
        return pltpu.make_async_remote_copy(
            src_ref=piece,
            dst_ref=piece,
            send_sem=extra_send.at[d],
            recv_sem=extra_recv.at[d],
            device_id=ring_id[d],
            device_id_type=MESH,
        )

    def all_bytes(s, rows, sem, count=2 * n_items):
        ref, lanes = [
            (wqkv, wqkv.shape[1]),
            (wout, None),
            (wup, up_half),
            (wup, up_half),
            (wdn, None),
            (wdn, None),
        ][s]
        if lanes is None:
            half = count // 2
            whole = ref.at[0:half, 0 : 2 * rows, :]
        else:
            whole = ref.at[0 : count * rows, 0:lanes]
        return pltpu.make_async_copy(whole, whole, sem)

    def x_wait(s):
        all_bytes(s, streams[s][2][0], x_recv.at[s]).wait()

    head_cols = wq_hbm.shape[1]
    own = [
        pltpu.make_async_copy(
            wq_hbm,
            wqkv.at[pl.ds(pl.multiple_of(fs * qkv_rows, UNIT), qkv_rows), 0:head_cols],
            local_sem.at[0],
        ),
        pltpu.make_async_copy(
            wk_hbm,
            wqkv.at[
                pl.ds(pl.multiple_of(fs * qkv_rows, UNIT), qkv_rows), head_cols : 2 * head_cols
            ],
            local_sem.at[1],
        ),
        pltpu.make_async_copy(
            wv_hbm,
            wqkv.at[pl.ds(pl.multiple_of(fs * qkv_rows, UNIT), qkv_rows), 2 * head_cols :],
            local_sem.at[2],
        ),
        pltpu.make_async_copy(tok_hbm, tok.at[tp], local_sem.at[3]),
        pltpu.make_async_copy(out_hbm, wout.at[fs], local_sem.at[4]),
        pltpu.make_async_copy(
            up_hbm,
            wup.at[pl.ds(pl.multiple_of(fs * up_rows, UNIT), up_rows), :],
            local_sem.at[5],
        ),
        pltpu.make_async_copy(down_hbm, wdn.at[fs], local_sem.at[6]),
    ]
    small = [
        pltpu.make_async_copy(src, dst, small_sem.at[n])
        for n, (src, dst) in enumerate(
            (
                (pre_gain_hbm, pre_gain),
                (first_hbm, first_ref),
                (second_hbm, second_ref),
                (bias_hbm, bias_ref),
                (surge_hbm, surge_ref),
                (head_gain_hbm, head_gain),
                (post_gain_hbm, post_gain),
                (mid_gain_hbm, mid_gain),
                (last_gain_hbm, last_gain),
            )
        )
    ]
    for copy in (*own[:4], *small, *own[4:]):
        copy.start()

    barrier = pltpu.get_barrier_semaphore()
    for target in (*ring_id, x_id, core_id):
        pl.semaphore_signal(barrier, inc=1, device_id=target, device_id_type=MESH)
    pl.semaphore_wait(barrier, 4)

    for copy in own[:3]:
        copy.wait()
    begin(QKV)

    def core_copy(k, src, dst):
        return pltpu.make_async_remote_copy(
            src_ref=src,
            dst_ref=dst,
            send_sem=core_send.at[k],
            recv_sem=core_recv.at[k],
            device_id=core_id,
            device_id_type=MESH,
        )

    own[3].wait()
    swap_tok = core_copy(0, tok.at[tp], tok.at[tp])
    swap_tok.start()
    for copy in (*small, *own[4:]):
        copy.wait()
    core_copy(0, tok.at[1 - tp], tok.at[1 - tp]).wait_recv()

    def norm_rows(gain, count, part=0, parts=1):
        def body(r, carry):
            at = pl.ds(pl.multiple_of(r * count, count), count)
            left = tok[0, at, :].astype(jnp.float32)
            right = tok[1, at, :].astype(jnp.float32)
            total = jnp.sum(left * left, axis=1, keepdims=True) + jnp.sum(
                right * right, axis=1, keepdims=True
            )
            scale = lax.rsqrt(total / width + EPS)
            normed[at, 0:dh] = (left * scale * gain[:, 0:dh]).astype(jnp.bfloat16)
            normed[at, dh:] = (right * scale * gain[:, dh:]).astype(jnp.bfloat16)
            return carry

        span = tokens // count // parts
        lax.fori_loop(part * span, (part + 1) * span, body, 0)

    norm_rows(pre_gain, 64)
    poll(QKV, 0)

    def rank_body(r, carry):
        at = pl.ds(pl.multiple_of(r * 256, 256), 256)
        rank[at, :] = lax.dot_general(
            normed[at, :],
            first_ref[...],
            (((1,), (1,)), ((), ())),
            preferred_element_type=jnp.float32,
        ).astype(jnp.bfloat16)
        return carry

    lax.fori_loop(0, tokens // 256, rank_body, 0)
    for i in range(1, n_items):
        poll(QKV, i)
        if i == n_items - 3:
            begin(OUT)

    for i in range(n_items):
        poll(OUT, i)
        if i == n_items - 3:
            begin(UP0)
    x_wait(QKV)

    chunks = tokens // CHUNK

    def attention_chunk(chunk, carry):
        @pl.when(chunk < n_items)
        def _():
            poll(UP0, chunk)

        @pl.when(chunk == n_items - 3)
        def _():
            begin(UP1)

        @pl.when(lax.rem(chunk, LENGTH // CHUNK) == 0)
        def _():
            state[...] = jnp.zeros_like(state)

        at = pl.ds(pl.multiple_of(chunk * CHUNK, CHUNK), CHUNK)
        surge_row = surge_ref[:, pl.ds(pl.multiple_of(chunk * CHUNK, CHUNK), CHUNK)]
        surge = jnp.transpose(jnp.broadcast_to(surge_row, (8, CHUNK)))[:, 0:1]
        qkv = jnp.dot(
            normed[at, :], wqkv[...], preferred_element_type=jnp.float32
        ).astype(jnp.bfloat16)
        mixed[at, :] = attend(
            qkv[:, 0:head_cols],
            qkv[:, head_cols : 2 * head_cols],
            qkv[:, 2 * head_cols :],
            rank[at, :],
            second_ref[...],
            bias_ref[...],
            surge,
            head_gain[...],
            state,
        )
        return carry

    lax.fori_loop(0, chunks, attention_chunk, 0)

    poll(UP1, 0)
    x_wait(OUT)

    def out_rows_body(r, carry):
        at = pl.ds(pl.multiple_of(r * 256, 256), 256)
        rows = mixed[at, :]
        for k in range(per_half):
            keep[at, k * cols : (k + 1) * cols] = jnp.dot(
                rows, wout[tp * per_half + k], preferred_element_type=jnp.float32
            ).astype(jnp.bfloat16)
            sendb[at, k * cols : (k + 1) * cols] = jnp.dot(
                rows, wout[(1 - tp) * per_half + k], preferred_element_type=jnp.float32
            ).astype(jnp.bfloat16)
        return carry

    row_blocks = tokens // 256
    lax.fori_loop(0, row_blocks // 2, out_rows_body, 0)
    poll(UP1, 1)
    lax.fori_loop(row_blocks // 2, row_blocks, out_rows_body, 0)
    core_copy(1, sendb, recvb).start()
    poll(UP1, 2)
    core_copy(1, sendb, recvb).wait_recv()

    def attn_rows(r, count):
        at = pl.ds(pl.multiple_of(r * count, count), count)
        return at, keep[at, :].astype(jnp.float32) + recvb[at, :].astype(jnp.float32)

    def square_body(r, carry):
        at, attn = attn_rows(r, 64)
        ss[at, :] = jnp.broadcast_to(
            jnp.sum(attn * attn, axis=1, keepdims=True), (64, ss.shape[1])
        )
        return carry

    lax.fori_loop(0, tokens // 64, square_body, 0)
    core_copy(2, ss, ss_in).start()
    poll(UP1, 3)
    core_copy(2, ss, ss_in).wait_recv()

    def resid_body(r, carry):
        at, attn = attn_rows(r, 64)
        total = ss[at, 0:1] + ss_in[at, 0:1]
        scale = lax.rsqrt(total / width + EPS)
        tok[tp, at, :] = (
            tok[tp, at, :].astype(jnp.float32) + attn * scale * post_gain[...]
        ).astype(jnp.bfloat16)
        return carry

    swap_tok.wait_send()
    lax.fori_loop(0, tokens // 64, resid_body, 0)
    swap_resid = core_copy(3, tok.at[tp], tok.at[tp])
    swap_resid.start()
    poll(UP1, 4)
    begin(DN0)
    core_copy(3, tok.at[1 - tp], tok.at[1 - tp]).wait_recv()
    norm_rows(mid_gain, 64, 0, 2)
    poll(UP1, 5)
    norm_rows(mid_gain, 64, 1, 2)
    poll(UP1, 6)

    blocks = 8
    hidden_cols = wup.shape[1] // blocks

    def up_body(b, carry):
        @pl.when(b < n_items)
        def _():
            poll(DN0, b)

        @pl.when(b == n_items - 3)
        def _():
            begin(DN1)

        @pl.when(b == 1)
        def _():
            x_wait(UP0)
            x_wait(UP1)

        @pl.when(b >= 1)
        def _():
            lanes = pl.ds(pl.multiple_of((b - 1) * hidden_cols, hidden_cols), hidden_cols)
            for r in range(tokens // 256):
                at = slice(r * 256, (r + 1) * 256)
                hidden = jnp.maximum(
                    jnp.dot(normed[at, :], wup[:, lanes], preferred_element_type=jnp.float32),
                    0.0,
                )
                sq[at, lanes] = (hidden * hidden).astype(jnp.bfloat16)

        return carry

    lax.fori_loop(0, blocks + 1, up_body, 0)

    def feed_copy(t):
        j, _, _ = shard_of(t)
        return pltpu.make_async_remote_copy(
            src_ref=fbuf.at[j],
            dst_ref=rbuf.at[j],
            send_sem=feed_send.at[t],
            recv_sem=feed_recv.at[t],
            device_id=core_id,
            device_id_type=MESH,
        )

    def shard_of(t):
        h = (t + 1) // 2
        d = 1 - lax.rem(t, 2)
        return shard_at(place - sign(d) * h), d, h

    def down_of(t):
        j, _, _ = shard_of(t)

        def body(r, carry):
            at = pl.ds(pl.multiple_of(r * 512, 512), 512)
            fbuf[j, at, :] = jnp.dot(
                sq[at, :], wdn[j], preferred_element_type=jnp.float32
            ).astype(jnp.bfloat16)
            return carry

        lax.fori_loop(0, tokens // 512, body, 0)

    def feed_rows(j, at):
        return fbuf[j, at, :].astype(jnp.float32) + rbuf[j, at, :].astype(jnp.float32)

    def lane_squares(feed):
        lanes = ss.shape[1]
        parts = [feed[:, k : k + lanes] for k in range(0, feed.shape[1], lanes)]
        return sum(part * part for part in parts)

    def squares_of(t):
        j, _, _ = shard_of(t)
        feed_copy(t).wait_recv()

        def body(r, carry):
            at = pl.ds(pl.multiple_of(r * 256, 256), 256)
            ss[at, :] += lane_squares(feed_rows(j, at))
            return carry

        lax.fori_loop(0, tokens // 256, body, 0)

    def last_x(d, e, h):
        x_copy(DN1, d, e, h, False).wait_recv()

    far = half_ring - 1

    def down_body(i, carry):
        poll(DN1, i)

        @pl.when(i == 2)
        def _():
            x_wait(DN0)

        @pl.when((i >= 2) & (i < n_items - 1))
        def _():
            _, d, h = shard_of(i - 1)
            last_x(d, 0, h)
            last_x(d, 1, h)

        @pl.when(i == n_items - 1)
        def _():
            last_x(0, 1, far)

        @pl.when(i != 1)
        def _():
            down_of(jnp.maximum(i - 1, 0))

        @pl.when(i == n_items - 2)
        def _():
            for d in range(2):
                last_x(d, 0, far)
                extra_copy(d, True).start()

        @pl.when((i == 1) | (i >= 3))
        def _():
            feed_copy(jnp.maximum(i - 2, 0)).start()

        @pl.when(i >= 3)
        def _():
            squares_of(i - 3)

        return carry

    core_copy(2, ss, ss_in).wait_send()
    ss[...] = jnp.zeros_like(ss)
    lax.fori_loop(0, n_items, down_body, 0)
    feed_copy(n_fs - 3).start()
    squares_of(n_fs - 4)
    last_x(1, 1, far)
    down_of(n_fs - 2)
    squares_of(n_fs - 3)
    feed_copy(n_fs - 2).start()
    for d in range(2):
        extra_copy(d, False).wait_recv()
    last_shard, _, _ = shard_of(n_fs - 1)
    count = tokens // LAST_BLOCKS

    def last_copy(q):
        at = pl.ds(q * count, count)
        return pltpu.make_async_remote_copy(
            src_ref=fbuf.at[last_shard, at, :],
            dst_ref=rbuf.at[last_shard, at, :],
            send_sem=last_send.at[q],
            recv_sem=last_recv.at[q],
            device_id=core_id,
            device_id_type=MESH,
        )

    for q in range(LAST_BLOCKS):
        at = pl.ds(q * count, count)
        fbuf[last_shard, at, :] = jnp.dot(
            sq[at, :], wdn[last_shard], preferred_element_type=jnp.float32
        ).astype(jnp.bfloat16)
        if q == 0:
            squares_of(n_fs - 2)
        last_copy(q).start()

    def last_body(r, carry):
        at = pl.ds(pl.multiple_of(r * 128, 128), 128)
        total = jnp.sum(
            ss[at, :] + lane_squares(feed_rows(last_shard, at)), axis=1, keepdims=True
        )
        scale = lax.rsqrt(total / width + EPS)
        for k in range(per_half):
            lanes = slice(k * cols, (k + 1) * cols)
            feed = feed_rows(tp * per_half + k, at)
            o_ref[at, lanes] = (
                tok[tp, at, lanes].astype(jnp.float32) + feed * scale * last_gain[:, lanes]
            ).astype(jnp.bfloat16)
        return carry

    for q in range(LAST_BLOCKS):
        last_copy(q).wait_recv()
        lax.fori_loop(q * count // 128, (q + 1) * count // 128, last_body, 0)

    for s in range(len(streams)):
        a, c = streams[s][2]
        all_bytes(s, a + c, ring_send.at[s]).wait()
        all_bytes(s, a, x_send.at[s], 2 * n_items - 2 * (s == DN1)).wait()
    for d in range(2):
        extra_copy(d, True).wait_send()
    swap_resid.wait_send()
    for t in range(n_fs - 1):
        feed_copy(t).wait_send()
    for q in range(LAST_BLOCKS):
        last_copy(q).wait_send()
    core_copy(1, sendb, recvb).wait_send()


def fused_layer(
    n_rep,
    n_fs,
    n_tp,
    tokens,
    attention_pre_gain,
    query_matrix,
    key_matrix,
    value_matrix,
    decay_first_weight,
    decay_second_weight,
    decay_offset_bias,
    extra_log_surge,
    readout_head_gain,
    output_matrix,
    attention_post_gain,
    feedforward_pre_gain,
    up_matrix,
    down_matrix,
    feedforward_post_gain,
):
    rows, dh = tokens.shape
    width = dh * n_tp
    qkv_cols = query_matrix.shape[1] + key_matrix.shape[1] + value_matrix.shape[1]
    hidden = up_matrix.shape[1]
    cols = down_matrix.shape[1]
    bf = jnp.bfloat16
    any_spec = pl.BlockSpec(memory_space=pl.ANY)
    dma = pltpu.SemaphoreType.DMA
    small = (
        attention_pre_gain[None, :],
        decay_first_weight.T,
        decay_second_weight,
        decay_offset_bias[None, :],
        extra_log_surge.T,
        readout_head_gain[None, :],
        attention_post_gain[None, :],
        feedforward_pre_gain[None, :],
        feedforward_post_gain[None, :],
    )
    return pl.pallas_call(
        functools.partial(layer_kernel, {"fs": n_fs}),
        out_shape=pltpu.VMEM((rows, dh), bf),
        in_specs=[any_spec] * 16,
        out_specs=pl.BlockSpec(memory_space=pltpu.VMEM),
        scratch_shapes=[
            pltpu.VMEM((width, qkv_cols), bf),
            pltpu.VMEM((n_fs, output_matrix.shape[0], cols), bf),
            pltpu.VMEM((width, hidden), bf),
            pltpu.VMEM((n_fs, hidden, cols), bf),
            pltpu.VMEM((n_tp, rows, dh), bf),
            pltpu.VMEM((rows, width), bf),
            pltpu.VMEM((rows, decay_first_weight.shape[1]), bf),
            pltpu.VMEM((rows, DV), bf),
            pltpu.VMEM((rows, dh), bf),
            pltpu.VMEM((rows, dh), bf),
            pltpu.VMEM((rows, dh), bf),
            pltpu.VMEM((rows, 128), jnp.float32),
            pltpu.VMEM((rows, 128), jnp.float32),
            pltpu.VMEM((rows, hidden), bf),
            pltpu.VMEM((n_fs, rows, cols), bf),
            pltpu.VMEM((n_fs, rows, cols), bf),
            pltpu.VMEM((DV, KEY_WIDTH), jnp.float32),
            *[pltpu.VMEM(a.shape, a.dtype) for a in small],
            dma((7,)),
            dma((len(small),)),
            dma((LAST_BLOCKS,)),
            dma((LAST_BLOCKS,)),
            dma((6,)),
            dma((2, 2, 2, n_fs // 2)),
            dma((6,)),
            dma((5,)),
            dma((2, 2, n_fs // 2)),
            dma((2,)),
            dma((2,)),
            dma((4,)),
            dma((4,)),
            dma((n_fs,)),
            dma((n_fs,)),
        ],
        compiler_params=pltpu.CompilerParams(
            collective_id=0, has_side_effects=True, vmem_limit_bytes=60 * 2**20
        ),
        name="layer",
    )(
        tokens,
        small[0],
        query_matrix,
        key_matrix,
        value_matrix,
        *small[1:6],
        output_matrix,
        *small[6:8],
        up_matrix,
        down_matrix,
        small[8],
    )


def per_device(n_rep, n_fs, n_tp, *args):
    tokens, query, second, out, up, down = args[0], args[2], args[6], args[10], args[13], args[14]
    fits = (
        n_rep == 2
        and n_tp == 2
        and n_fs % 2 == 0
        and 6 <= n_fs <= 8
        and tokens.shape[0] % LENGTH == 0
        and tokens.shape[0] // CHUNK == n_fs
        and second.shape[1] == KEY_WIDTH
        and out.shape[1] % 128 == 0
        and query.shape[0] % (8 * UNIT) == 0
        and up.shape[0] % (8 * UNIT) == 0
        and down.shape[1] == out.shape[1]
    )
    return (fused_layer if fits else on_device)(n_rep, n_fs, n_tp, *args)


def solution(mesh):
    return jax.shard_map(
        functools.partial(per_device, mesh.shape["rep"], mesh.shape["fs"], mesh.shape["tp"]),
        mesh=mesh,
        in_specs=(
            P(("rep", "fs"), "tp"),
            P(),
            P("fs", "tp"),
            P("fs", "tp"),
            P("fs", "tp"),
            P(),
            P(None, "tp"),
            P("tp"),
            P(("rep", "fs"), "tp"),
            P(),
            P("tp", "fs"),
            P("tp"),
            P(),
            P("fs", "tp"),
            P("tp", "fs"),
            P("tp"),
        ),
        out_specs=P(("rep", "fs"), "tp"),
        check_vma=False,
    )
```
